128 devices in a mesh: sp: 16 (over z, y), dp: 8 (over x, core).
Axes of the slice: x: 4, y: 4, z: 4, core: 2. Of those that a mesh axis runs over, the one named last changes fastest.
Arguments:
- residual: bfloat16 [8, 2048, 2048], P('dp', 'sp'), may hold values from -6 to 6
- query: bfloat16 [8, 2048, 16, 128], P('dp', 'sp'), may hold values from -6 to 6
- key_value: bfloat16 [8, 2048, 16, 128], P('dp', 'sp'), may hold values from -6 to 6
- out_weight: bfloat16 [2048, 2048], P(None, 'dp'), may hold values from -0.125 to 0.125
- norm_gain: float32 [2048], replicated, may hold values from 0.1 to 1.9
- query_gain: float32 [64], replicated, may hold values from 1.5 to 4.5
- key_gain: float32 [64], replicated, may hold values from 1.5 to 4.5
- route_ids: int32 [8, 2048, 4], P('dp', 'sp'), may hold values from 0 to 127, all different within a row; in each aligned block of 128 rows (0 to 127, 128 to 255, ..., all dimensions but the last counted through in order) at most 6 rows name the same one
- route_weights: float32 [8, 2048, 4], P('dp', 'sp'), may hold values from 0.2 to 1
- shared_gate: bfloat16 [2048, 512], replicated, may hold values from -0.125 to 0.125
- shared_up: bfloat16 [2048, 512], replicated, may hold values from -0.125 to 0.125
- shared_down: bfloat16 [512, 2048], replicated, may hold values from -0.25 to 0.25
- expert_gate: bfloat16 [128, 2048, 512], P(('sp', 'dp')), may hold values from -0.125 to 0.125
- expert_up: bfloat16 [128, 2048, 512], P(('sp', 'dp')), may hold values from -0.125 to 0.125
- expert_down: bfloat16 [128, 512, 2048], P(('sp', 'dp')), may hold values from -0.25 to 0.25
Outputs:
- result: bfloat16 [8, 2048, 2048], P('dp', 'sp')
The draws below stay inside these ranges and needn't reach their ends.
Inputs may be any that keep to these rules, and one draw needn't show every extreme that they name: `route_ids`: each row names 4 different experts. Among the rows of one device no expert is named more than 6 times, a bound that some block reaches.
All inputs are finite; a program needn't handle non-finite values.
Results may differ from the reference program's by a relative error of at most 0.014.
The reference program's roundings to bfloat16 on the way count: a program that leaves them out, or rounds other values in their place, can miss the bound.
Values may be sent and summed in bfloat16 or wider, within the bound.
No kernel may reach another device: no remote copies, remote signals or barrier semaphores. Data moves between devices by JAX's collectives and lax.ppermute only.
A program may use at most 128 MiB of HBM per device.

```python
import math
import jax
import jax.numpy as jnp
import numpy as np
from jax import lax

D = 2048
HD = 64
Q_HEADS = 32
KV_HEADS = 16
REP = 2
GRID_W = 64
EFF = 512
SFF = 512
EXPERTS = 128
TOP_K = 4
TOK_DEV = 128
LEN = 2048
SEQS = 8
CAP = 6
N_SP = 16
N_DP = 8


def key_base_draw(key):
    drawn = jax.random.normal(jax.random.fold_in(key, 11), (SEQS, LEN, KV_HEADS, HD), jnp.float32)
    return jnp.clip(drawn, -6.0, 6.0)


def draw_query(key, part):
    drawn = jax.random.normal(jax.random.fold_in(key, 21), (SEQS, LEN, KV_HEADS, REP * HD), jnp.float32)
    drawn = jnp.clip(drawn, -6.0, 6.0)
    return drawn.astype(jnp.bfloat16)


def draw_key_value(key, part):
    key_base = key_base_draw(key)
    values = jax.random.normal(jax.random.fold_in(key, 12), (SEQS, LEN, KV_HEADS, HD), jnp.float32)
    values = jnp.clip(values, -6.0, 6.0)
    return jnp.concatenate([key_base, values], axis=-1).astype(jnp.bfloat16)


def gain_draw(key, salt):
    spread = jax.random.uniform(jax.random.fold_in(key, salt), (HD,), jnp.float32, jnp.log(1.5), jnp.log(3.0))
    return jnp.exp(spread)


def draw_query_gain(key, part):
    return gain_draw(key, 31)


def draw_key_gain(key, part):
    return gain_draw(key, 32)


def level_of(stream_key, extent, cuts, smallest, high):
    factor_of, own = 1.0, jax.random.fold_in(stream_key, 6)
    for axis_at, shards_of in cuts:
        draws = jnp.exp(jax.random.uniform(jax.random.fold_in(own, axis_at), (shards_of,), jnp.float32, smallest / len(cuts), high / len(cuts)))
        factor_of = factor_of * jnp.repeat(draws, extent[axis_at] // shards_of).reshape([-1 if axis == axis_at else 1 for axis in range(len(extent))])
    return factor_of


def routed_block(rng, own, number, rows, amount, top, bound, lean):
    order = jax.random.permutation(rng, amount)
    crowded, usual = load_shares(amount, rows * top, bound, lean, True), load_shares(amount, rows * top, bound, lean, False)
    places = jnp.arange(amount)

    def named(lengths, turn):
        used = int((lengths > 0).sum())
        fixed = max(1, used // 4)
        moved = fixed + (places - fixed + turn * (used - fixed)) % max(1, amount - fixed)
        return jnp.zeros((amount,), jnp.int32).at[order[jnp.where(places < fixed, places, moved)]].set(jnp.asarray(lengths, jnp.int32))

    lengths = jnp.where(number % 4 == 0, named(crowded, number // 4), named(usual, number - number // 4 - 1))
    mixed = jax.random.permutation(jax.random.fold_in(own, 3), amount)
    donor, receiver = mixed[0:amount // 2 * 2:2], mixed[1:amount // 2 * 2:2]
    margin = jnp.minimum(lengths[donor] - 1, bound - lengths[receiver]) // 2
    margin = jnp.where((donor == order[0]) | (receiver == order[0]) | (lengths[receiver] == 0), 0, jnp.maximum(margin, 0))
    moved = jax.random.randint(jax.random.fold_in(own, 4), (amount // 2,), 0, 1 << 20) % (margin + 1)
    lengths = lengths.at[donor].add(-moved).at[receiver].add(moved)
    labels = jnp.searchsorted(jnp.cumsum(lengths), jnp.arange(rows * top), side="right").astype(jnp.int32)
    listing = labels.reshape(top, rows).T
    listing = listing[jax.random.permutation(jax.random.fold_in(own, 1), rows)]
    turn = jax.random.randint(jax.random.fold_in(own, 2), (rows, 1), 0, top)
    return jnp.take_along_axis(listing, (jnp.arange(top)[None, :] + turn) % top, axis=1)


def load_shares(count, total, limit, skew, full):
    loads = [(1 << 20) // math.isqrt(standing ** skew) + 1 for standing in range(1, count + 1)]
    largest = limit if full else min(limit, max(-(-total // count), total * loads[0] // sum(loads)))
    least = 1 if total - largest >= count - 1 else 0
    given, rest = [largest] + [least] * (count - 1), total - largest - least * (count - 1)
    while rest > 0:
        movable = [i for i in range(1, count) if given[i] < largest] or [i for i in range(1, count) if given[i] < limit]
        pool, left = sum([loads[i] for i in movable]), rest
        for i in movable:
            more = min(limit - given[i], max(1, left * loads[i] // pool), rest)
            given[i] = given[i] + more
            rest = rest - more
    return np.array(given)


def normal_values(rng, dims, scale, limit, cuts=(), held_as=jnp.bfloat16):
    entries = jax.random.normal(rng, dims, jnp.float32) * scale
    if len(cuts) > 0:
        entries = level_of(rng, dims, cuts, -0.22, 0.18) * entries
    return jnp.clip(entries, min=-limit, max=limit).astype(held_as)


def setup_inputs(seed: int = 0) -> dict:
    splits = jax.random.split(jax.random.key(seed), 16)
    residual = normal_values(splits[0], (SEQS, LEN, D), 1.0, 6.0, ((0, 8), (1, 16)))
    query = draw_query(jax.random.fold_in(splits[15], 71), 0)
    key_value = draw_key_value(jax.random.fold_in(splits[15], 71), 0)
    out_weight = normal_values(splits[3], (Q_HEADS * HD, D), (Q_HEADS * HD) ** -0.5, 0.125, ((1, 8),))
    norm_gain = jnp.clip(1.0 + 0.18 * jax.random.normal(splits[4], (D,), jnp.float32), 0.1, 1.9)
    query_gain = draw_query_gain(jax.random.fold_in(splits[15], 71), 0)
    key_gain = draw_key_gain(jax.random.fold_in(splits[15], 71), 0)
    route_ids_keys = jax.random.split(jax.random.fold_in(splits[7], 1), SEQS * LEN // TOK_DEV)
    route_ids_turns = jax.random.permutation(jax.random.fold_in(splits[7], 3), SEQS * LEN // TOK_DEV)
    route_ids = jax.vmap(lambda own, number: routed_block(jax.random.fold_in(splits[7], 2), own, number, TOK_DEV, EXPERTS, TOP_K, CAP, 2))(route_ids_keys, route_ids_turns).reshape((SEQS, LEN, TOP_K))
    route_weights = jnp.clip(jnp.exp(math.log(1.0) - 1.609438 * jax.random.uniform(splits[8], (SEQS, LEN, TOP_K), jnp.float32) ** level_of(splits[8], (SEQS, LEN, TOP_K), ((0, 8), (1, 16)), -0.2, 0.2)), 0.2, 1.0)
    shared_gate = normal_values(splits[9], (D, SFF), D ** -0.5, 0.125)
    shared_up = normal_values(splits[10], (D, SFF), D ** -0.5, 0.125)
    shared_down = normal_values(splits[11], (SFF, D), SFF ** -0.5, 0.25)
    expert_gate = normal_values(splits[12], (EXPERTS, D, EFF), D ** -0.5, 0.125, ((0, 128),))
    expert_up = normal_values(splits[13], (EXPERTS, D, EFF), D ** -0.5, 0.125, ((0, 128),))
    expert_down = normal_values(splits[14], (EXPERTS, EFF, D), EFF ** -0.5, 0.25, ((0, 128),))
    return {"residual": residual, "query": query, "key_value": key_value, "out_weight": out_weight, "norm_gain": norm_gain, "query_gain": query_gain, "key_gain": key_gain, "route_ids": route_ids, "route_weights": route_weights, "shared_gate": shared_gate, "shared_up": shared_up, "shared_down": shared_down, "expert_gate": expert_gate, "expert_up": expert_up, "expert_down": expert_down}


norm_eps = 1e-06
rope_theta = 10000.0
routed_scale = 2.5

def rotate_half(values, position, half_width):
    inverse_freq = rope_theta ** (-jnp.arange(0, half_width, 2, dtype=jnp.float32) / half_width)
    angles = position.astype(jnp.float32)[:, None] * inverse_freq[None, :]
    angles = jnp.concatenate([angles, angles], axis=-1)
    cosine = jnp.cos(angles)[:, None, :]
    sine_part = jnp.sin(angles)[:, None, :]
    first_half, second = jnp.split(values, 2, axis=-1)
    turned = jnp.concatenate([-second, first_half], axis=-1)
    return values * cosine + turned * sine_part

def prepare(values, gain_vector, grid_row, grid_col):
    head_dim = values.shape[-1]
    floats = values.astype(jnp.float32)
    normed = floats * lax.rsqrt(lax.optimization_barrier(jnp.mean(floats * floats, axis=-1, keepdims=True)) + norm_eps)
    normed = normed * gain_vector.astype(jnp.float32)
    half_width = head_dim // 2
    turned = jnp.concatenate([rotate_half(normed[..., :half_width], grid_row, half_width), rotate_half(normed[..., half_width:], grid_col, half_width)], axis=-1)
    return turned.astype(jnp.bfloat16)

def attend(queries, key_rows, values):
    length, groups, repeats, head_dim = queries.shape
    block_rows = min(512, length)
    score_scale = head_dim ** (-0.5)

    def one_block(query_block):
        scores = jnp.einsum('qgrd,kgd->grqk', query_block.astype(jnp.float32), key_rows.astype(jnp.float32)) * score_scale
        row_max = lax.optimization_barrier(jnp.max(scores, axis=-1, keepdims=True))
        weights = jnp.exp(scores - row_max)
        row_total = lax.optimization_barrier(jnp.sum(weights, axis=-1, keepdims=True))
        rounded = weights.astype(jnp.bfloat16)
        mixed = jnp.einsum('grqk,kgd->grqd', rounded.astype(jnp.float32), values.astype(jnp.float32)) / row_total
        return jnp.transpose(mixed, (2, 0, 1, 3)).astype(jnp.bfloat16)
    blocks = queries.reshape(length // block_rows, block_rows, groups, repeats, head_dim)
    return lax.map(one_block, blocks).reshape(length, groups * repeats * head_dim)

def swiglu(row_block, gate_weight, up_weight, down_weight):
    gate_part = jnp.dot(row_block, gate_weight, preferred_element_type=jnp.float32)
    up_part = jnp.dot(row_block, up_weight, preferred_element_type=jnp.float32)
    hidden = (jax.nn.silu(gate_part) * up_part).astype(jnp.bfloat16)
    return jnp.dot(hidden, down_weight, preferred_element_type=jnp.float32)

def sequence_mixer(res_rows, query_rows, pair_rows, out_weight, norm_gain, query_gain, key_gain):
    length = query_rows.shape[0]
    kv_heads = query_rows.shape[1]
    head_dim = pair_rows.shape[2] // 2
    repeats = query_rows.shape[2] // head_dim
    position = jnp.arange(length, dtype=jnp.int32)
    grid_row = position // GRID_W
    grid_col = position % GRID_W
    queries = prepare(query_rows.reshape(length, kv_heads * repeats, head_dim), query_gain, grid_row, grid_col)
    queries = queries.reshape(length, kv_heads, repeats, head_dim)
    key_rows = prepare(pair_rows[..., :head_dim], key_gain, grid_row, grid_col)
    values = pair_rows[..., head_dim:]
    attention = attend(queries, key_rows, values)
    mixed = res_rows.astype(jnp.float32) + jnp.dot(attention, out_weight, preferred_element_type=jnp.float32)
    normed = mixed * lax.rsqrt(lax.optimization_barrier(jnp.mean(mixed * mixed, axis=-1, keepdims=True)) + norm_eps)
    normed = (normed * norm_gain.astype(jnp.float32)).astype(jnp.bfloat16)
    return (mixed, normed)

def reference(residual, query, key_value, out_weight, norm_gain, query_gain, key_gain, route_ids, route_weights, shared_gate, shared_up, shared_down, expert_gate, expert_up, expert_down):

    def one_sequence(items):
        return sequence_mixer(items[0], items[1], items[2], out_weight, norm_gain, query_gain, key_gain)
    mixed, normed = lax.map(one_sequence, (residual, query, key_value))
    model_width = residual.shape[-1]
    flat_normed = normed.reshape(-1, model_width)
    token_count = flat_normed.shape[0]
    shared = swiglu(flat_normed, shared_gate, shared_up, shared_down)
    route_list = route_ids.reshape(token_count, -1)
    raw_weights = route_weights.reshape(token_count, -1).astype(jnp.float32)
    gate_values = raw_weights / lax.optimization_barrier(jnp.sum(raw_weights, axis=-1, keepdims=True)) * routed_scale
    padded_rows = jnp.concatenate([flat_normed, jnp.zeros((1, model_width), jnp.bfloat16)], axis=0)
    most_rows = CAP * N_SP * N_DP

    def one_expert(totals, expert_id):
        hit_mask = route_list == expert_id
        weight = lax.optimization_barrier(jnp.sum(jnp.where(hit_mask, gate_values, jnp.zeros_like(gate_values)), axis=-1))
        chosen = jnp.nonzero(jnp.any(hit_mask, axis=-1), size=most_rows, fill_value=token_count)[0]
        chosen = chosen.astype(jnp.int32)
        row_block = padded_rows[chosen]
        output = swiglu(row_block, expert_gate[expert_id], expert_up[expert_id], expert_down[expert_id]).astype(jnp.bfloat16)
        weight_pad = jnp.concatenate([weight, jnp.zeros((1,), jnp.float32)], axis=0)
        totals = totals.at[chosen].add(output.astype(jnp.float32) * weight_pad[chosen][:, None])
        return (totals, None)
    routed, _ = lax.scan(one_expert, jnp.zeros((token_count + 1, model_width), jnp.float32), jnp.arange(EXPERTS, dtype=jnp.int32))
    combined = mixed.reshape(token_count, model_width) + shared + routed[:token_count]
    return combined.astype(jnp.bfloat16).reshape(residual.shape)
```

```python
import jax
import jax.numpy as jnp
import numpy as np
from jax import lax
from jax.experimental import pallas as pl
from jax.experimental.pallas import tpu as pltpu
from jax.sharding import PartitionSpec as P

GRID_W = 64
HD = 64
EPS = 1e-06
THETA = 10000.0
ROUTED_SCALE = 2.5
CAP = 6
PAIRS = CAP // 2
QUARTERS = 4
F32 = jnp.float32
BF16 = jnp.bfloat16


def iota(shape, axis):
    return lax.broadcasted_iota(jnp.int32, shape, axis)


def rotary_tables(query_gain, key_gain, first_token, tokens):
    lane = np.arange(128)
    half = (lane % HD) // 32
    freq = (THETA ** (-(2.0 * (lane % 16)) / 32.0)).astype(np.float32)
    position = first_token + jnp.arange(tokens, dtype=jnp.int32)
    row = (position // GRID_W).astype(F32)[:, None]
    col = (position % GRID_W).astype(F32)[:, None]
    angle = jnp.where(half[None, :] == 0, row, col) * freq[None, :]
    cosine, sine = jnp.cos(angle), jnp.sin(angle)
    lower = (lane % 32) < 16
    up, down = (lane + 16) % HD, (lane - 16) % HD

    def tables(gain, scale):
        pair = jnp.concatenate([gain, gain]) * scale
        return (
            pair[None, :] * cosine,
            jnp.where(lower, -gain[up] * scale, 0.0)[None, :] * sine,
            jnp.where(lower, 0.0, gain[down] * scale)[None, :] * sine,
        )

    is_key = (lane < HD)[None, :]
    q_own, q_up, q_down = tables(query_gain, HD**-0.5)
    k_own, k_up, k_down = tables(key_gain, 1.0)
    k_own = jnp.where(is_key, k_own, 1.0)
    k_up = jnp.where(is_key, k_up, 0.0)
    k_down = jnp.where(is_key, k_down, 0.0)
    return jnp.stack([q_own, q_up, q_down, k_own, k_up, k_down])


def prepare_kernel(q_ref, kv_ref, table_ref, out_ref):
    heads = q_ref.shape[0]
    block = (iota((128, 128), 0) // HD == iota((128, 128), 1) // HD).astype(F32).astype(BF16)
    is_key = iota((1, 128), 1) < HD

    def turned(x, base, keys):
        square = x * x
        high = square.astype(BF16)
        low = (square - high.astype(F32)).astype(BF16)
        total = jnp.dot(high, block, preferred_element_type=F32)
        total = total + jnp.dot(low, block, preferred_element_type=F32)
        scale = lax.rsqrt(total * (1.0 / HD) + EPS)
        if keys:
            scale = jnp.where(is_key, scale, 1.0)
        mixed = (
            x * table_ref[base]
            + pltpu.roll(x, 112, 1) * table_ref[base + 1]
            + pltpu.roll(x, 16, 1) * table_ref[base + 2]
        )
        return (mixed * scale).astype(BF16)

    for h in range(heads):
        out_ref[h, :, :128] = turned(q_ref[h].astype(F32), 0, False)
        out_ref[h, :, 128:] = turned(kv_ref[h].astype(F32), 3, True)


def prepare(query, pair, tables):
    heads, tokens, width = query.shape
    step = 4
    return pl.pallas_call(
        prepare_kernel,
        grid=(heads // step,),
        in_specs=[
            pl.BlockSpec((step, tokens, width), lambda i: (i, 0, 0)),
            pl.BlockSpec((step, tokens, width), lambda i: (i, 0, 0)),
            pl.BlockSpec(tables.shape, lambda i: (0, 0, 0)),
        ],
        out_specs=pl.BlockSpec((step, tokens, 2 * width), lambda i: (i, 0, 0)),
        out_shape=jax.ShapeDtypeStruct((heads, tokens, 2 * width), BF16),
        name="prepare",
    )(query, pair, tables)


def attend_kernel(q_ref, kv_ref, out_ref, keys_ref, values_ref):
    @pl.when(pl.program_id(0) == 0)
    def _():
        key = kv_ref[:, 128 : 128 + HD]
        value = kv_ref[:, 128 + HD :]
        keys_ref[...] = jnp.concatenate([key, key], axis=1)
        values_ref[...] = jnp.concatenate([value, value], axis=1)

    first = iota((1, 128), 1) < HD
    query = q_ref[...]
    outs = []
    for head in range(2):
        mine = jnp.where(first if head == 0 else ~first, query, jnp.zeros_like(query))
        scores = lax.dot_general(
            mine, keys_ref[...], (((1,), (1,)), ((), ())), preferred_element_type=F32
        )
        weights = jnp.exp(scores - jnp.max(scores, axis=-1, keepdims=True))
        total = jnp.sum(weights, axis=-1, keepdims=True)
        mixed = jnp.dot(weights.astype(BF16), values_ref[...], preferred_element_type=F32)
        outs.append(mixed / total)
    out_ref[...] = jnp.where(first, outs[0], outs[1]).astype(BF16)


def attend(rows):
    length, width = rows.shape
    block = 256
    return pl.pallas_call(
        attend_kernel,
        grid=(length // block,),
        in_specs=[
            pl.BlockSpec((block, 128), lambda i: (i, 0)),
            pl.BlockSpec((length, width), lambda i: (0, 0)),
        ],
        out_specs=pl.BlockSpec((block, 128), lambda i: (i, 0)),
        out_shape=jax.ShapeDtypeStruct((length, 128), BF16),
        scratch_shapes=[pltpu.VMEM((length, 128), BF16), pltpu.VMEM((length, 128), BF16)],
        name="attend",
    )(rows, rows)


def route_kernel(ids_ref, weights_ref, place_ref, gates_ref):
    tokens, top = ids_ref.shape
    experts = place_ref.shape[0] // CAP
    expert = iota((tokens, experts), 1)
    hits = [(ids_ref[:, k : k + 1] == expert).astype(F32) for k in range(top)]
    used = sum(hits[1:], hits[0])
    earlier = (iota((tokens, tokens), 1) < iota((tokens, tokens), 0)).astype(F32).astype(BF16)
    before = jnp.dot(earlier, used.astype(BF16), preferred_element_type=F32)
    raw = weights_ref[...]
    gate = raw / jnp.sum(raw, axis=-1, keepdims=True) * ROUTED_SCALE
    slots = iota((tokens, experts * CAP), 1)
    place = jnp.zeros((tokens, experts * CAP), F32)
    gated = jnp.zeros((tokens, experts * CAP), F32)
    for k in range(top):
        rank = jnp.sum(hits[k] * before, axis=-1, keepdims=True).astype(jnp.int32)
        slot = (rank // 2) * (2 * experts) + ids_ref[:, k : k + 1] * 2 + rank % 2
        here = slots == slot
        place = jnp.where(here, 1.0, place)
        gated = jnp.where(here, gate[:, k : k + 1], gated)
    place_ref[...] = jnp.transpose(place).astype(BF16)
    gates_ref[...] = gated


def route(ids, weights, experts):
    tokens, top = ids.shape
    return pl.pallas_call(
        route_kernel,
        out_shape=(
            jax.ShapeDtypeStruct((experts * CAP, tokens), BF16),
            jax.ShapeDtypeStruct((tokens, experts * CAP), F32),
        ),
        name="route",
    )(ids, weights)


def wire_permutation(transposed):
    wire = iota((128, 128), 1 if transposed else 0)
    flat = iota((128, 128), 0 if transposed else 1)
    source = (wire // 2 % QUARTERS) * 32 + (wire // 8) * 2 + wire % 2
    return (flat == source).astype(F32).astype(BF16)


def fold(rows, write):
    permute = wire_permutation(False)
    part = rows.shape[1] // QUARTERS
    for g in range(rows.shape[0] // 32):
        stacked = jnp.concatenate(
            [rows[g * 32 : (g + 1) * 32, q * part : (q + 1) * part] for q in range(QUARTERS)], axis=0
        )
        write(g, jnp.dot(permute, stacked, preferred_element_type=F32).astype(BF16))


def unfold(wire_ref, rows_ref):
    permute = wire_permutation(True)
    part = wire_ref.shape[1]
    for g in range(wire_ref.shape[0] // 128):
        block = jnp.dot(
            permute, wire_ref[g * 128 : (g + 1) * 128, :], preferred_element_type=F32
        ).astype(BF16)
        for q in range(QUARTERS):
            rows_ref[g * 32 : (g + 1) * 32, q * part : (q + 1) * part] = block[q * 32 : (q + 1) * 32]


def project_kernel(columns_ref, heads_ref, *refs):
    pieces = refs[:9]
    residual_ref, gain_ref, place_ref, mixed_ref, normed_ref, wire_ref = refs[9:15]
    weight_ref, part_ref, sems = refs[15:]
    half = weight_ref.shape[1] // 2
    targets = [weight_ref.at[s] for s in range(7)] + [
        weight_ref.at[7, pl.ds(0, half)],
        weight_ref.at[7, pl.ds(half, half)],
    ]
    copies = [
        pltpu.make_async_copy(pieces[s], targets[s], sems.at[s]) for s in range(9)
    ]
    for copy in copies:
        copy.start()
    rows = jnp.concatenate([heads_ref[h] for h in range(heads_ref.shape[0])], axis=1)
    for s in range(8):
        copies[s].wait()
        if s == 7:
            copies[8].wait()
        part_ref[columns_ref[s]] = jnp.dot(rows, weight_ref[s], preferred_element_type=F32)
    width = part_ref.shape[2]
    square = None
    for j in range(8):
        block = part_ref[j] + residual_ref[:, j * width : (j + 1) * width].astype(F32)
        mixed_ref[:, j * width : (j + 1) * width] = block
        part = jnp.sum(block * block, axis=-1, keepdims=True)
        square = part if square is None else square + part
    scale = lax.rsqrt(square * (1.0 / (8 * width)) + EPS)
    normed = (mixed_ref[...] * scale * gain_ref[...]).astype(BF16)
    normed_ref[...] = normed
    span = place_ref.shape[0] // PAIRS
    part = normed.shape[1] // QUARTERS
    for c in range(PAIRS):
        slots = jnp.dot(
            place_ref[c * span : (c + 1) * span, :], normed, preferred_element_type=F32
        ).astype(BF16)

        def write(g, block):
            wire_ref[g * 128 : (g + 1) * 128, c * part : (c + 1) * part] = block

        fold(slots, write)


def project(columns, heads, pieces, residual, gain, place):
    tokens, width = residual.shape
    peers = place.shape[0] // CAP
    vmem = pl.BlockSpec(memory_space=pltpu.VMEM)
    return pl.pallas_call(
        project_kernel,
        in_specs=[pl.BlockSpec(memory_space=pltpu.SMEM), vmem]
        + [pl.BlockSpec(memory_space=pl.ANY)] * 9
        + [vmem] * 3,
        out_specs=[vmem] * 3,
        out_shape=(
            jax.ShapeDtypeStruct((tokens, width), F32),
            jax.ShapeDtypeStruct((tokens, width), BF16),
            jax.ShapeDtypeStruct((peers * 8, width * CAP // 8), BF16),
        ),
        scratch_shapes=[
            pltpu.VMEM((8,) + pieces[0].shape, BF16),
            pltpu.VMEM((8, tokens, width // 8), F32),
            pltpu.SemaphoreType.DMA((9,)),
        ],
        name="project",
    )(columns, heads, *pieces, residual, gain, place)


def expert_kernel(wire_ref, gate_ref, up_ref, down_ref, out_ref, rows_ref):
    unfold(wire_ref, rows_ref)
    rows = rows_ref[...]
    gate = jnp.dot(rows, gate_ref[...], preferred_element_type=F32)
    up = jnp.dot(rows, up_ref[...], preferred_element_type=F32)
    hidden = (gate / (1.0 + jnp.exp(-gate)) * up).astype(BF16)
    output = jnp.dot(hidden, down_ref[...], preferred_element_type=F32).astype(BF16)

    def write(g, block):
        out_ref[g * 128 : (g + 1) * 128, :] = block

    fold(output, write)


def expert(wire, gate, up, down):
    rows, width = wire.shape
    part = width // PAIRS

    def whole(array):
        return pl.BlockSpec(array.shape, lambda c: (0, 0))

    return pl.pallas_call(
        expert_kernel,
        grid=(PAIRS,),
        in_specs=[pl.BlockSpec((rows, part), lambda c: (0, c)), whole(gate), whole(up), whole(down)],
        out_specs=pl.BlockSpec((rows, part), lambda c: (0, c)),
        out_shape=jax.ShapeDtypeStruct(wire.shape, BF16),
        scratch_shapes=[pltpu.VMEM((rows // QUARTERS, part * QUARTERS), BF16)],
        name="expert",
    )(wire, gate, up, down)


def combine_kernel(wire_ref, gates_ref, mixed_ref, shared_ref, out_ref, rows_ref, total_ref):
    c = pl.program_id(0)
    unfold(wire_ref, rows_ref)
    gates = gates_ref[...]
    tokens = gates.shape[0]
    high = gates.astype(BF16)
    rest = gates - high.astype(F32)
    middle = rest.astype(BF16)
    low = (rest - middle.astype(F32)).astype(BF16)
    parts = jnp.dot(
        jnp.concatenate([high, middle, low], axis=0), rows_ref[...], preferred_element_type=F32
    )
    routed = parts[:tokens] + (parts[tokens : 2 * tokens] + parts[2 * tokens :])

    @pl.when(c == 0)
    def _():
        total_ref[...] = routed

    @pl.when(c > 0)
    def _():
        total_ref[...] = total_ref[...] + routed

    @pl.when(c == pl.num_programs(0) - 1)
    def _():
        out_ref[...] = (mixed_ref[...] + shared_ref[...] + total_ref[...]).astype(BF16)


def combine(wire, gates, mixed, shared):
    rows, width = wire.shape
    tokens = mixed.shape[0]
    part = width // PAIRS

    def whole(array):
        return pl.BlockSpec(array.shape, lambda c: (0, 0))

    return pl.pallas_call(
        combine_kernel,
        grid=(PAIRS,),
        in_specs=[
            pl.BlockSpec((rows, part), lambda c: (0, c)),
            pl.BlockSpec((tokens, gates.shape[1] // PAIRS), lambda c: (0, c)),
            whole(mixed),
            whole(shared),
        ],
        out_specs=pl.BlockSpec(mixed.shape, lambda c: (0, 0)),
        out_shape=jax.ShapeDtypeStruct(mixed.shape, BF16),
        scratch_shapes=[
            pltpu.VMEM((rows // QUARTERS, part * QUARTERS), BF16),
            pltpu.VMEM(mixed.shape, F32),
        ],
        name="combine",
    )(wire, gates, mixed, shared)


def swiglu(row_block, gate_weight, up_weight, down_weight):
    gate_part = jnp.dot(row_block, gate_weight, preferred_element_type=F32)
    up_part = jnp.dot(row_block, up_weight, preferred_element_type=F32)
    hidden = (jax.nn.silu(gate_part) * up_part).astype(BF16)
    return jnp.dot(hidden, down_weight, preferred_element_type=F32)


def shift(values, target):
    size = lax.axis_size("dp")
    pairs = [(d, 2 * (target(d // 2, d % 2)[0] % (size // 2)) + target(d // 2, d % 2)[1]) for d in range(size)]
    return lax.ppermute(values, "dp", pairs)


def right(x, core):
    return x + 1, core


def left(x, core):
    return x - 1, core


def partner(x, core):
    return x, 1 - core


def per_device(
    residual,
    query,
    key_value,
    out_weight,
    norm_gain,
    query_gain,
    key_gain,
    route_ids,
    route_weights,
    shared_gate,
    shared_up,
    shared_down,
    expert_gate,
    expert_up,
    expert_down,
):
    tokens, width = residual.shape[1:]
    experts = expert_gate.shape[0] * lax.axis_size(("sp", "dp"))
    ring = lax.axis_size("dp") // 2
    half = out_weight.shape[0] // 2

    from_left = shift(out_weight, right)
    from_right = shift(out_weight, left)
    own_pair = shift(out_weight, partner)

    tables = rotary_tables(query_gain, key_gain, lax.axis_index("sp") * tokens, tokens)
    outgoing = prepare(
        jnp.transpose(query[0], (1, 0, 2)), jnp.transpose(key_value[0], (1, 0, 2)), tables
    )
    rows = lax.all_to_all(outgoing, "sp", split_axis=0, concat_axis=0, tiled=True)
    place, gates = route(route_ids[0], route_weights[0], experts)

    rows, from_left, from_right = lax.optimization_barrier((rows, from_left, from_right))
    far_top = shift(from_left[:half], right)
    far_bottom = shift(from_right[half:], left)
    left_pair = shift(from_left, partner)
    right_pair = shift(from_right, partner)
    attention = attend(rows.reshape(-1, rows.shape[2]))
    attention, far_top, far_bottom = lax.optimization_barrier((attention, far_top, far_bottom))
    far_top_pair = shift(far_top, partner)
    far_bottom_pair = shift(far_bottom, partner)
    heads = lax.all_to_all(
        attention.reshape(-1, tokens, attention.shape[1]), "sp", split_axis=0, concat_axis=0, tiled=True
    )

    me = lax.axis_index("dp")
    x, core = me // 2, me % 2

    def column(dx, flip):
        return 2 * ((x + dx) % ring) + (1 - core if flip else core)

    columns = jnp.stack(
        [
            column(0, False),
            column(0, True),
            column(-1, False),
            column(1, False),
            column(-1, True),
            column(1, True),
            column(2, False),
            column(2, True),
        ]
    ).astype(jnp.int32)
    far = jnp.concatenate([far_top, far_bottom], axis=0)
    pieces = [
        out_weight,
        own_pair,
        from_left,
        from_right,
        left_pair,
        right_pair,
        far,
        far_top_pair,
        far_bottom_pair,
    ]
    mixed, normed, wire = project(
        columns, heads, pieces, residual[0], norm_gain.reshape(1, -1), place
    )
    wire_shape = (wire.shape[0] // 8, 8, wire.shape[1])

    def exchange(values):
        return lax.all_to_all(
            values.reshape(wire_shape), ("sp", "dp"), split_axis=0, concat_axis=0, tiled=True
        ).reshape(values.shape)

    arrived = exchange(wire)
    shared = swiglu(normed, shared_gate, shared_up, shared_down)
    output = expert(arrived, expert_gate[0], expert_up[0], expert_down[0])
    returned = exchange(output)
    return combine(returned, gates, mixed, shared).reshape(1, tokens, width)


def solution(mesh):
    in_specs = (
        P("dp", "sp", None),
        P("dp", "sp", None, None),
        P("dp", "sp", None, None),
        P(None, "dp"),
        P(),
        P(),
        P(),
        P("dp", "sp", None),
        P("dp", "sp", None),
        P(),
        P(),
        P(),
        P(("sp", "dp"), None, None),
        P(("sp", "dp"), None, None),
        P(("sp", "dp"), None, None),
    )
    out_specs = P("dp", "sp", None)
    return jax.shard_map(
        per_device, mesh=mesh, in_specs=in_specs, out_specs=out_specs, check_vma=False
    )
```

```python
import jax
import jax.numpy as jnp
import numpy as np
from jax import lax
from jax.experimental import pallas as pl
from jax.experimental.pallas import tpu as pltpu
from jax.sharding import PartitionSpec as P

GRID_W = 64
HD = 64
EPS = 1e-06
THETA = 10000.0
ROUTED_SCALE = 2.5
CAP = 6
PAIRS = CAP // 2
QUARTERS = 4
F32 = jnp.float32
BF16 = jnp.bfloat16


def iota(shape, axis):
    return lax.broadcasted_iota(jnp.int32, shape, axis)


LANES = 2 * HD


def local(values):
    return pltpu.with_memory_space_constraint(values, pltpu.VMEM)


def distant(values):
    return pltpu.with_memory_space_constraint(values, pltpu.HBM)


def limit(mib):
    return pltpu.CompilerParams(vmem_limit_bytes=mib * 2**20)


def angle_tables(tokens, blocks):
    lane = np.arange(LANES)
    by_row = lane % HD < HD // 2
    freq = THETA ** (-(2.0 * (lane % (HD // 4))) / (HD // 2))
    col = (np.arange(tokens) % GRID_W)[:, None] * freq[None, :]
    row = np.arange(blocks * tokens // GRID_W)[:, None] * freq[None, :]
    col = np.where(by_row, 0.0, np.stack([np.cos(col), np.sin(col)]))
    row = np.where(by_row, np.stack([np.cos(row), np.sin(row)]), 0.0)
    row = row.reshape(2, blocks, tokens // GRID_W, LANES).transpose(1, 0, 2, 3)
    return col.astype(np.float32), row.astype(np.float32)


def prepare_kernel(
    block_ref, q_ref, kv_ref, col_ref, row_ref, q_gain_ref, k_gain_ref, out_ref, table_ref
):
    del block_ref
    tokens, heads = q_ref.shape[:2]
    shape = (tokens, LANES)
    lane = iota(shape, 1)
    is_key = lane < HD
    block = (iota((LANES, LANES), 0) // HD == iota((LANES, LANES), 1) // HD).astype(F32).astype(BF16)

    @pl.when(pl.program_id(0) == 0)
    def _():
        lower = lane % (HD // 2) < HD // 4

        def angles(which):
            rows = [
                col_ref[which, r * GRID_W : (r + 1) * GRID_W, :] + row_ref[0, which, r : r + 1, :]
                for r in range(tokens // GRID_W)
            ]
            return jnp.concatenate(rows, axis=0)

        cosine, sine = angles(0), angles(1)

        def tables(gain_ref, scale):
            gain = gain_ref[...] * scale
            gain = jnp.broadcast_to(jnp.concatenate([gain, gain], axis=1), shape)
            up = pltpu.roll(gain, LANES - HD // 4, 1)
            down = pltpu.roll(gain, HD // 4, 1)
            return (
                gain * cosine,
                jnp.where(lower, -up * sine, 0.0),
                jnp.where(lower, 0.0, down * sine),
            )

        for i, table in enumerate(tables(q_gain_ref, HD**-0.5)):
            table_ref[i] = table
        own, up, down = tables(k_gain_ref, 1.0)
        table_ref[3] = jnp.where(is_key, own, 1.0)
        table_ref[4] = jnp.where(is_key, up, 0.0)
        table_ref[5] = jnp.where(is_key, down, 0.0)

    def turned(x, base, keys):
        square = x * x
        high = square.astype(BF16)
        low = (square - high.astype(F32)).astype(BF16)
        total = jnp.dot(high, block, preferred_element_type=F32)
        total = total + jnp.dot(low, block, preferred_element_type=F32)
        scale = lax.rsqrt(total * (1.0 / HD) + EPS)
        if keys:
            scale = jnp.where(is_key, scale, 1.0)
        mixed = (
            x * table_ref[base]
            + pltpu.roll(x, LANES - HD // 4, 1) * table_ref[base + 1]
            + pltpu.roll(x, HD // 4, 1) * table_ref[base + 2]
        )
        return (mixed * scale).astype(BF16)

    query = jnp.swapaxes(q_ref[...].astype(F32), 0, 1)
    pair = jnp.swapaxes(kv_ref[...].astype(F32), 0, 1)
    for h in range(heads):
        out_ref[h, :, :LANES] = turned(query[h], 0, False)
        out_ref[h, :, LANES:] = turned(pair[h], 3, True)


def prepare(query, pair, query_gain, key_gain, block, blocks):
    tokens, heads, width = query.shape
    step = 8
    col, row = angle_tables(tokens, blocks)
    gains = [gain.reshape(1, -1) for gain in (query_gain, key_gain)]
    return pl.pallas_call(
        prepare_kernel,
        grid_spec=pltpu.PrefetchScalarGridSpec(
            num_scalar_prefetch=1,
            grid=(heads // step,),
            in_specs=[
                pl.BlockSpec((tokens, step, width), lambda i, b: (0, i, 0)),
                pl.BlockSpec((tokens, step, width), lambda i, b: (0, i, 0)),
                pl.BlockSpec(col.shape, lambda i, b: (0, 0, 0)),
                pl.BlockSpec((1,) + row.shape[1:], lambda i, b: (b[0], 0, 0, 0)),
                pl.BlockSpec((1, HD), lambda i, b: (0, 0)),
                pl.BlockSpec((1, HD), lambda i, b: (0, 0)),
            ],
            out_specs=pl.BlockSpec((step, tokens, 2 * width), lambda i, b: (i, 0, 0)),
            scratch_shapes=[pltpu.VMEM((6, tokens, width), F32)],
        ),
        out_shape=jax.ShapeDtypeStruct((heads, tokens, 2 * width), BF16),
        compiler_params=limit(16),
        name="prepare",
    )(jnp.full((1,), block, jnp.int32), query, pair, col, row, *gains)


def attend_kernel(q_ref, kv_ref, out_ref, keys_ref, values_ref):
    @pl.when(pl.program_id(0) == 0)
    def _():
        key = kv_ref[:, 128 : 128 + HD]
        value = kv_ref[:, 128 + HD :]
        keys_ref[...] = jnp.concatenate([key, key], axis=1)
        values_ref[:, :128] = jnp.concatenate([value, value], axis=1)
        values_ref[:, 128:] = jnp.ones_like(values_ref[:, 128:])

    first = iota((1, 128), 1) < HD
    block = 512
    parts = [(r, head) for r in range(q_ref.shape[0] // block) for head in range(2)]

    def score(part):
        r, head = part
        query = q_ref[r * block : (r + 1) * block, :]
        mine = jnp.where(first if head == 0 else ~first, query, jnp.zeros_like(query))
        return lax.dot_general(
            mine, keys_ref[...], (((1,), (1,)), ((), ())), preferred_element_type=F32
        )

    def mix(scores):
        weights = jnp.exp(scores - jnp.max(scores, axis=-1, keepdims=True)).astype(BF16)
        mixed = jnp.dot(weights, values_ref[...], preferred_element_type=F32)
        return mixed[:, :128] / mixed[:, 128:]

    outs = []
    ahead = score(parts[0])
    for n in range(len(parts)):
        scores = ahead
        if n + 1 < len(parts):
            ahead = score(parts[n + 1])
        outs.append(mix(scores))
    for r in range(len(parts) // 2):
        out_ref[r * block : (r + 1) * block, :] = jnp.where(
            first, outs[2 * r], outs[2 * r + 1]
        ).astype(BF16)


def attend(rows):
    length, width = rows.shape
    block = 512
    return pl.pallas_call(
        attend_kernel,
        grid=(length // block,),
        in_specs=[
            pl.BlockSpec((block, 128), lambda i: (i, 0)),
            pl.BlockSpec((length, width), lambda i: (0, 0)),
        ],
        out_specs=pl.BlockSpec((block, 128), lambda i: (i, 0)),
        out_shape=pltpu.HBM((length, 128), BF16),
        scratch_shapes=[pltpu.VMEM((length, 128), BF16), pltpu.VMEM((length, 256), BF16)],
        compiler_params=limit(32),
        name="attend",
    )(rows, rows)


def route_kernel(ids_ref, weights_ref, place_ref, gates_ref):
    tokens, top = ids_ref.shape
    experts = place_ref.shape[0] // CAP
    expert = iota((tokens, experts), 1)
    hits = [(ids_ref[:, k : k + 1] == expert).astype(F32) for k in range(top)]
    used = sum(hits[1:], hits[0])
    earlier = (iota((tokens, tokens), 1) < iota((tokens, tokens), 0)).astype(F32).astype(BF16)
    before = jnp.dot(earlier, used.astype(BF16), preferred_element_type=F32)
    raw = weights_ref[...]
    gate = raw / jnp.sum(raw, axis=-1, keepdims=True) * ROUTED_SCALE
    slots = iota((tokens, experts * CAP), 1)
    place = jnp.zeros((tokens, experts * CAP), F32)
    gated = jnp.zeros((tokens, experts * CAP), F32)
    for k in range(top):
        rank = jnp.sum(hits[k] * before, axis=-1, keepdims=True).astype(jnp.int32)
        slot = (rank // 2) * (2 * experts) + ids_ref[:, k : k + 1] * 2 + rank % 2
        here = slots == slot
        place = jnp.where(here, 1.0, place)
        gated = jnp.where(here, gate[:, k : k + 1], gated)
    place_ref[...] = jnp.transpose(place).astype(BF16)
    gates_ref[...] = gated


def route(ids, weights, experts):
    tokens, top = ids.shape
    return pl.pallas_call(
        route_kernel,
        out_shape=(
            pltpu.VMEM((experts * CAP, tokens), BF16),
            pltpu.VMEM((tokens, experts * CAP), F32),
        ),
        compiler_params=limit(8),
        name="route",
    )(ids, weights)


def wire_permutation(transposed):
    wire = iota((128, 128), 1 if transposed else 0)
    flat = iota((128, 128), 0 if transposed else 1)
    source = (wire // 2 % QUARTERS) * 32 + (wire // 8) * 2 + wire % 2
    return (flat == source).astype(F32).astype(BF16)


def fold(rows, write):
    permute = wire_permutation(False)
    part = rows.shape[1] // QUARTERS
    for g in range(rows.shape[0] // 32):
        stacked = jnp.concatenate(
            [rows[g * 32 : (g + 1) * 32, q * part : (q + 1) * part] for q in range(QUARTERS)], axis=0
        )
        write(g, jnp.dot(permute, stacked, preferred_element_type=F32).astype(BF16))


def unfold(wire_ref, rows_ref):
    permute = wire_permutation(True)
    part = wire_ref.shape[1]
    for g in range(wire_ref.shape[0] // 128):
        block = jnp.dot(
            permute, wire_ref[g * 128 : (g + 1) * 128, :], preferred_element_type=F32
        ).astype(BF16)
        for q in range(QUARTERS):
            rows_ref[g * 32 : (g + 1) * 32, q * part : (q + 1) * part] = block[q * 32 : (q + 1) * 32]


def project_kernel(columns_ref, heads_ref, *refs):
    pieces = refs[:8]
    residual_hbm, gain_ref, place_ref, mixed_hbm, normed_hbm, wire_ref = refs[8:14]
    weight_ref, residual_ref, part_ref, mixed_ref, normed_ref, sems = refs[14:]
    copies = [
        pltpu.make_async_copy(pieces[s], weight_ref.at[s], sems.at[s]) for s in range(8)
    ]
    copies.append(pltpu.make_async_copy(residual_hbm, residual_ref, sems.at[8]))
    copies.append(pltpu.make_async_copy(mixed_ref, mixed_hbm, sems.at[9]))
    copies.append(pltpu.make_async_copy(normed_ref, normed_hbm, sems.at[10]))
    for copy in copies[:9]:
        copy.start()
    rows = jnp.concatenate([heads_ref[h] for h in range(heads_ref.shape[0])], axis=1)
    for s in range(8):
        copies[s].wait()
        part_ref[columns_ref[s]] = jnp.dot(rows, weight_ref[s], preferred_element_type=F32)
    copies[8].wait()
    width = part_ref.shape[2]
    square = None
    for j in range(8):
        block = part_ref[j] + residual_ref[:, j * width : (j + 1) * width].astype(F32)
        mixed_ref[:, j * width : (j + 1) * width] = block
        part = jnp.sum(block * block, axis=-1, keepdims=True)
        square = part if square is None else square + part
    scale = lax.rsqrt(square * (1.0 / (8 * width)) + EPS)
    normed = (mixed_ref[...] * scale * gain_ref[...]).astype(BF16)
    normed_ref[...] = normed
    copies[9].start()
    copies[10].start()
    span = place_ref.shape[0] // PAIRS
    part = normed.shape[1] // QUARTERS
    for c in range(PAIRS):
        slots = jnp.dot(
            place_ref[c * span : (c + 1) * span, :], normed, preferred_element_type=F32
        ).astype(BF16)

        def write(g, block):
            wire_ref[g * 128 : (g + 1) * 128, c * part : (c + 1) * part] = block

        fold(slots, write)
    copies[9].wait()
    copies[10].wait()


def project(columns, heads, pieces, residual, gain, place):
    tokens, width = residual.shape
    peers = place.shape[0] // CAP
    vmem = pl.BlockSpec(memory_space=pltpu.VMEM)
    return pl.pallas_call(
        project_kernel,
        in_specs=[pl.BlockSpec(memory_space=pltpu.SMEM), vmem]
        + [pl.BlockSpec(memory_space=pl.ANY)] * 9
        + [vmem] * 2,
        out_specs=[pl.BlockSpec(memory_space=pl.ANY)] * 2 + [vmem],
        out_shape=(
            pltpu.HBM((tokens, width), F32),
            pltpu.HBM((tokens, width), BF16),
            pltpu.VMEM((peers * 8, width * CAP // 8), BF16),
        ),
        scratch_shapes=[
            pltpu.VMEM((8,) + pieces[0].shape, BF16),
            pltpu.VMEM(residual.shape, BF16),
            pltpu.VMEM((8, tokens, width // 8), F32),
            pltpu.VMEM((tokens, width), F32),
            pltpu.VMEM((tokens, width), BF16),
            pltpu.SemaphoreType.DMA((11,)),
        ],
        compiler_params=limit(32),
        name="project",
    )(
        columns,
        local(heads),
        *(distant(piece) for piece in pieces),
        distant(residual),
        gain,
        local(place),
    )


def expert_kernel(wire_ref, gate_ref, up_ref, down_ref, out_hbm, rows_ref, out_ref, sems):
    part = wire_ref.shape[1] // PAIRS
    span = rows_ref.shape[0] // PAIRS
    for c in range(PAIRS):
        unfold(
            wire_ref.at[:, pl.ds(c * part, part)], rows_ref.at[pl.ds(c * span, span)]
        )
    rows = rows_ref[...]
    gate = jnp.dot(rows, gate_ref[...], preferred_element_type=F32)
    up = jnp.dot(rows, up_ref[...], preferred_element_type=F32)
    hidden = (gate / (1.0 + jnp.exp(-gate)) * up).astype(BF16)
    copies = []
    for c in range(PAIRS):
        output = jnp.dot(
            hidden[c * span : (c + 1) * span], down_ref[...], preferred_element_type=F32
        ).astype(BF16)

        def write(g, block):
            out_ref[g * 128 : (g + 1) * 128, c * part : (c + 1) * part] = block

        fold(output, write)
        lanes = pl.ds(c * part, part)
        copies.append(
            pltpu.make_async_copy(out_ref.at[:, lanes], out_hbm.at[:, lanes], sems.at[c])
        )
        copies[c].start()
    for copy in copies:
        copy.wait()


def expert(wire, gate, up, down):
    rows, width = wire.shape
    vmem = pl.BlockSpec(memory_space=pltpu.VMEM)
    return pl.pallas_call(
        expert_kernel,
        in_specs=[vmem] * 4,
        out_specs=pl.BlockSpec(memory_space=pl.ANY),
        out_shape=pltpu.HBM(wire.shape, BF16),
        scratch_shapes=[
            pltpu.VMEM((rows * CAP // 8, width * 8 // CAP), BF16),
            pltpu.VMEM(wire.shape, BF16),
            pltpu.SemaphoreType.DMA((PAIRS,)),
        ],
        compiler_params=limit(32),
        name="expert",
    )(local(wire), local(gate), local(up), local(down))


def shared_kernel(normed_ref, mixed_ref, gate_ref, up_ref, down_ref, out_ref):
    rows = normed_ref[...]
    gate = jnp.dot(rows, gate_ref[...], preferred_element_type=F32)
    up = jnp.dot(rows, up_ref[...], preferred_element_type=F32)
    hidden = (gate / (1.0 + jnp.exp(-gate)) * up).astype(BF16)
    output = jnp.dot(hidden, down_ref[...], preferred_element_type=F32)

    @pl.when(pl.program_id(0) == 0)
    def _():
        out_ref[...] = mixed_ref[...] + output

    @pl.when(pl.program_id(0) > 0)
    def _():
        out_ref[...] = out_ref[...] + output


def shared(normed, mixed, gate, up, down):
    block = 256

    def whole(array):
        return pl.BlockSpec(array.shape, lambda i: (0, 0))

    columns = pl.BlockSpec((gate.shape[0], block), lambda i: (0, i))
    return pl.pallas_call(
        shared_kernel,
        grid=(gate.shape[1] // block,),
        in_specs=[
            whole(normed),
            whole(mixed),
            columns,
            columns,
            pl.BlockSpec((block, down.shape[1]), lambda i: (i, 0)),
        ],
        out_specs=whole(mixed),
        out_shape=pltpu.HBM(mixed.shape, F32),
        compiler_params=limit(20),
        name="shared",
    )(*(distant(array) for array in (normed, mixed, gate, up, down)))


def combine_kernel(wire_ref, gates_ref, base_hbm, out_ref, rows_ref, base_ref, sem):
    copy = pltpu.make_async_copy(base_hbm, base_ref, sem)
    copy.start()
    gates = gates_ref[...]
    tokens = gates.shape[0]
    high = gates.astype(BF16)
    rest = gates - high.astype(F32)
    middle = rest.astype(BF16)
    low = (rest - middle.astype(F32)).astype(BF16)
    stacked = jnp.concatenate([high, middle, low], axis=0)
    part = wire_ref.shape[1] // PAIRS
    span = rows_ref.shape[0] // PAIRS
    for c in range(PAIRS):
        unfold(
            wire_ref.at[:, pl.ds(c * part, part)], rows_ref.at[pl.ds(c * span, span)]
        )
    copy.wait()
    block = 512
    for n in range(base_ref.shape[1] // block):
        lanes = slice(n * block, (n + 1) * block)
        parts = jnp.dot(stacked, rows_ref[:, lanes], preferred_element_type=F32)
        routed = parts[:tokens] + (parts[tokens : 2 * tokens] + parts[2 * tokens :])
        out_ref[:, lanes] = (base_ref[:, lanes] + routed).astype(BF16)


def combine(wire, gates, base):
    rows, width = wire.shape
    vmem = pl.BlockSpec(memory_space=pltpu.VMEM)
    return pl.pallas_call(
        combine_kernel,
        in_specs=[vmem, vmem, pl.BlockSpec(memory_space=pl.ANY)],
        out_specs=vmem,
        out_shape=jax.ShapeDtypeStruct(base.shape, BF16),
        scratch_shapes=[
            pltpu.VMEM((rows * CAP // 8, width * 8 // CAP), BF16),
            pltpu.VMEM(base.shape, F32),
            pltpu.SemaphoreType.DMA,
        ],
        compiler_params=limit(24),
        name="combine",
    )(local(wire), local(gates), distant(base))


def shift(values, target):
    size = lax.axis_size("dp")

    def place(d):
        x, core = target(d // 2, d % 2)
        return 2 * (x % (size // 2)) + core

    return lax.ppermute(values, "dp", [(d, place(d)) for d in range(size)])


def apart(x, core):
    return x + 1 - 2 * core, core


def across(x, core):
    return x - 1 + 2 * core, core


def partner(x, core):
    return x, 1 - core


def per_device(
    residual,
    query,
    key_value,
    out_weight,
    norm_gain,
    query_gain,
    key_gain,
    route_ids,
    route_weights,
    shared_gate,
    shared_up,
    shared_down,
    expert_gate,
    expert_up,
    expert_down,
):
    tokens, width = residual.shape[1:]
    experts = expert_gate.shape[0] * lax.axis_size(("sp", "dp"))
    ring = lax.axis_size("dp") // 2
    blocks = lax.axis_size("sp")

    near = shift(out_weight, apart)
    other = shift(out_weight, across)
    own_pair = shift(out_weight, partner)
    outgoing = prepare(
        query[0], key_value[0], query_gain, key_gain, lax.axis_index("sp"), blocks
    )
    rows = lax.all_to_all(outgoing, "sp", split_axis=0, concat_axis=0, tiled=True)
    rows, near, other = lax.optimization_barrier((rows, near, other))
    far = shift(near, apart)
    near_pair = shift(near, partner)
    other_pair = shift(other, partner)
    attention = attend(rows.reshape(-1, rows.shape[2]))
    far, ids, _ = lax.optimization_barrier((far, route_ids[0], attention))
    place, gates = route(ids, route_weights[0], experts)
    far_pair = shift(far, partner)
    heads = lax.all_to_all(
        attention.reshape(-1, tokens, attention.shape[1]), "sp", split_axis=0, concat_axis=0, tiled=True
    )

    me = lax.axis_index("dp")
    x, core = me // 2, me % 2
    away = 1 - 2 * core
    steps = jnp.array([0, 0, -1, 1, 1, -1, 2, 2], jnp.int32) * away
    flips = jnp.array([0, 1, 0, 0, 1, 1, 0, 1], jnp.int32)
    columns = 2 * ((x + steps) % ring) + (core + flips) % 2
    pieces = [out_weight, own_pair, near, other, near_pair, other_pair, far, far_pair]
    mixed, normed, wire = project(
        columns, heads, pieces, residual[0], norm_gain.reshape(1, -1), place
    )
    wire_shape = (wire.shape[0] // 8, 8, wire.shape[1])

    def exchange(values):
        return lax.all_to_all(
            values.reshape(wire_shape), ("sp", "dp"), split_axis=0, concat_axis=0, tiled=True
        ).reshape(values.shape)

    arrived = exchange(wire)
    base = shared(normed, mixed, shared_gate, shared_up, shared_down)
    output = expert(arrived, expert_gate[0], expert_up[0], expert_down[0])
    returned = exchange(output)
    return combine(returned, gates, base).reshape(1, tokens, width)


def solution(mesh):
    in_specs = (
        P("dp", "sp", None),
        P("dp", "sp", None, None),
        P("dp", "sp", None, None),
        P(None, "dp"),
        P(),
        P(),
        P(),
        P("dp", "sp", None),
        P("dp", "sp", None),
        P(),
        P(),
        P(),
        P(("sp", "dp"), None, None),
        P(("sp", "dp"), None, None),
        P(("sp", "dp"), None, None),
    )
    out_specs = P("dp", "sp", None)
    return jax.shard_map(
        per_device, mesh=mesh, in_specs=in_specs, out_specs=out_specs, check_vma=False
    )
```

```python
import jax
import jax.numpy as jnp
import numpy as np
from jax import lax
from jax.experimental import pallas as pl
from jax.experimental.pallas import tpu as pltpu
from jax.sharding import PartitionSpec as P


GRID_W = 64
HD = 64
EPS = 1e-06
THETA = 10000.0
ROUTED_SCALE = 2.5
CAP = 6
PAIRS = CAP // 2
QUARTERS = 4
F32 = jnp.float32
BF16 = jnp.bfloat16


def iota(shape, axis):
    return lax.broadcasted_iota(jnp.int32, shape, axis)


LANES = 2 * HD


def local(values):
    return pltpu.with_memory_space_constraint(values, pltpu.VMEM)


def distant(values):
    return pltpu.with_memory_space_constraint(values, pltpu.HBM)


def limit(mib):
    return pltpu.CompilerParams(vmem_limit_bytes=mib * 2**20)


def angle_tables(tokens, blocks):
    lane = np.arange(LANES)
    by_row = lane % HD < HD // 2
    freq = THETA ** (-(2.0 * (lane % (HD // 4))) / (HD // 2))
    col = (np.arange(tokens) % GRID_W)[:, None] * freq[None, :]
    row = np.arange(blocks * tokens // GRID_W)[:, None] * freq[None, :]
    col = np.where(by_row, 0.0, np.stack([np.cos(col), np.sin(col)]))
    row = np.where(by_row, np.stack([np.cos(row), np.sin(row)]), 0.0)
    row = row.reshape(2, blocks, tokens // GRID_W, LANES).transpose(1, 0, 2, 3)
    return col.astype(np.float32), row.astype(np.float32)


def prepare_kernel(
    block_ref, q_ref, kv_ref, col_ref, row_ref, q_gain_ref, k_gain_ref, out_ref, table_ref
):
    del block_ref
    tokens, heads = q_ref.shape[:2]
    shape = (tokens, LANES)
    lane = iota(shape, 1)
    is_key = lane < HD
    block = (iota((LANES, LANES), 0) // HD == iota((LANES, LANES), 1) // HD).astype(F32).astype(BF16)

    @pl.when(pl.program_id(0) == 0)
    def _():
        lower = lane % (HD // 2) < HD // 4

        def angles(which):
            rows = [
                col_ref[which, r * GRID_W : (r + 1) * GRID_W, :] + row_ref[0, which, r : r + 1, :]
                for r in range(tokens // GRID_W)
            ]
            return jnp.concatenate(rows, axis=0)

        cosine, sine = angles(0), angles(1)

        def tables(gain_ref, scale):
            gain = gain_ref[...] * scale
            gain = jnp.broadcast_to(jnp.concatenate([gain, gain], axis=1), shape)
            up = pltpu.roll(gain, LANES - HD // 4, 1)
            down = pltpu.roll(gain, HD // 4, 1)
            return (
                gain * cosine,
                jnp.where(lower, -up * sine, 0.0),
                jnp.where(lower, 0.0, down * sine),
            )

        for i, table in enumerate(tables(q_gain_ref, HD**-0.5)):
            table_ref[i] = table
        own, up, down = tables(k_gain_ref, 1.0)
        table_ref[3] = jnp.where(is_key, own, 1.0)
        table_ref[4] = jnp.where(is_key, up, 0.0)
        table_ref[5] = jnp.where(is_key, down, 0.0)

    def turned(x, base, keys):
        square = x * x
        high = square.astype(BF16)
        low = (square - high.astype(F32)).astype(BF16)
        total = jnp.dot(high, block, preferred_element_type=F32)
        total = total + jnp.dot(low, block, preferred_element_type=F32)
        scale = lax.rsqrt(total * (1.0 / HD) + EPS)
        if keys:
            scale = jnp.where(is_key, scale, 1.0)
        mixed = (
            x * table_ref[base]
            + pltpu.roll(x, LANES - HD // 4, 1) * table_ref[base + 1]
            + pltpu.roll(x, HD // 4, 1) * table_ref[base + 2]
        )
        return (mixed * scale).astype(BF16)

    query = jnp.swapaxes(q_ref[...].astype(F32), 0, 1)
    pair = jnp.swapaxes(kv_ref[...].astype(F32), 0, 1)
    for h in range(heads):
        out_ref[h, :, :LANES] = turned(query[h], 0, False)
        out_ref[h, :, LANES:] = turned(pair[h], 3, True)


def prepare(query, pair, query_gain, key_gain, block, blocks):
    tokens, heads, width = query.shape
    step = 8
    col, row = angle_tables(tokens, blocks)
    gains = [gain.reshape(1, -1) for gain in (query_gain, key_gain)]
    return pl.pallas_call(
        prepare_kernel,
        grid_spec=pltpu.PrefetchScalarGridSpec(
            num_scalar_prefetch=1,
            grid=(heads // step,),
            in_specs=[
                pl.BlockSpec((tokens, step, width), lambda i, b: (0, i, 0)),
                pl.BlockSpec((tokens, step, width), lambda i, b: (0, i, 0)),
                pl.BlockSpec(col.shape, lambda i, b: (0, 0, 0)),
                pl.BlockSpec((1,) + row.shape[1:], lambda i, b: (b[0], 0, 0, 0)),
                pl.BlockSpec((1, HD), lambda i, b: (0, 0)),
                pl.BlockSpec((1, HD), lambda i, b: (0, 0)),
            ],
            out_specs=pl.BlockSpec((step, tokens, 2 * width), lambda i, b: (i, 0, 0)),
            scratch_shapes=[pltpu.VMEM((6, tokens, width), F32)],
        ),
        out_shape=jax.ShapeDtypeStruct((heads, tokens, 2 * width), BF16),
        compiler_params=limit(16),
        name="prepare",
    )(
        jnp.full((1,), block, jnp.int32),
        *(distant(array) for array in (query, pair, jnp.asarray(col), jnp.asarray(row), *gains)),
    )


def attend_kernel(q_ref, kv_ref, out_ref, keys_ref, values_ref):
    @pl.when(pl.program_id(0) == 0)
    def _():
        key = kv_ref[:, 128 : 128 + HD]
        value = kv_ref[:, 128 + HD :]
        keys_ref[...] = jnp.concatenate([key, key], axis=1)
        values_ref[:, :128] = jnp.concatenate([value, value], axis=1)
        values_ref[:, 128:] = jnp.ones_like(values_ref[:, 128:])

    first = iota((1, 128), 1) < HD
    block = 512
    parts = [(r, head) for r in range(q_ref.shape[0] // block) for head in range(2)]

    def score(part):
        r, head = part
        query = q_ref[r * block : (r + 1) * block, :]
        mine = jnp.where(first if head == 0 else ~first, query, jnp.zeros_like(query))
        return lax.dot_general(
            mine, keys_ref[...], (((1,), (1,)), ((), ())), preferred_element_type=F32
        )

    def mix(scores):
        weights = jnp.exp(scores - jnp.max(scores, axis=-1, keepdims=True)).astype(BF16)
        mixed = jnp.dot(weights, values_ref[...], preferred_element_type=F32)
        return mixed[:, :128] / mixed[:, 128:]

    outs = []
    ahead = score(parts[0])
    for n in range(len(parts)):
        scores = ahead
        if n + 1 < len(parts):
            ahead = score(parts[n + 1])
        outs.append(mix(scores))
    for r in range(len(parts) // 2):
        out_ref[r * block : (r + 1) * block, :] = jnp.where(
            first, outs[2 * r], outs[2 * r + 1]
        ).astype(BF16)


def attend(rows):
    length, width = rows.shape
    block = 512
    return pl.pallas_call(
        attend_kernel,
        grid=(length // block,),
        in_specs=[
            pl.BlockSpec((block, 128), lambda i: (i, 0)),
            pl.BlockSpec((length, width), lambda i: (0, 0)),
        ],
        out_specs=pl.BlockSpec((block, 128), lambda i: (i, 0)),
        out_shape=pltpu.HBM((length, 128), BF16),
        scratch_shapes=[pltpu.VMEM((length, 128), BF16), pltpu.VMEM((length, 256), BF16)],
        compiler_params=limit(32),
        name="attend",
    )(rows, rows)


def route_kernel(ids_ref, weights_ref, place_ref, gates_ref):
    tokens, top = ids_ref.shape
    experts = place_ref.shape[0] // CAP
    expert = iota((tokens, experts), 1)
    hits = [(ids_ref[:, k : k + 1] == expert).astype(F32) for k in range(top)]
    used = sum(hits[1:], hits[0])
    earlier = (iota((tokens, tokens), 1) < iota((tokens, tokens), 0)).astype(F32).astype(BF16)
    before = jnp.dot(earlier, used.astype(BF16), preferred_element_type=F32)
    raw = weights_ref[...]
    gate = raw / jnp.sum(raw, axis=-1, keepdims=True) * ROUTED_SCALE
    slots = iota((tokens, experts * CAP), 1)
    place = jnp.zeros((tokens, experts * CAP), F32)
    gated = jnp.zeros((tokens, experts * CAP), F32)
    for k in range(top):
        rank = jnp.sum(hits[k] * before, axis=-1, keepdims=True).astype(jnp.int32)
        slot = (rank // 2) * (2 * experts) + ids_ref[:, k : k + 1] * 2 + rank % 2
        here = slots == slot
        place = jnp.where(here, 1.0, place)
        gated = jnp.where(here, gate[:, k : k + 1], gated)
    place_ref[...] = jnp.transpose(place).astype(BF16)
    gates_ref[...] = gated


def route(ids, weights, experts):
    tokens, _ = ids.shape
    return pl.pallas_call(
        route_kernel,
        out_shape=(
            pltpu.VMEM((experts * CAP, tokens), BF16),
            pltpu.VMEM((tokens, experts * CAP), F32),
        ),
        compiler_params=limit(8),
        name="route",
    )(ids, weights)


def wire_permutation(transposed):
    wire = iota((128, 128), 1 if transposed else 0)
    flat = iota((128, 128), 0 if transposed else 1)
    source = (wire // 2 % QUARTERS) * 32 + (wire // 8) * 2 + wire % 2
    return (flat == source).astype(F32).astype(BF16)


def fold(rows, write):
    permute = wire_permutation(False)
    part = rows.shape[1] // QUARTERS
    for g in range(rows.shape[0] // 32):
        stacked = jnp.concatenate(
            [rows[g * 32 : (g + 1) * 32, q * part : (q + 1) * part] for q in range(QUARTERS)], axis=0
        )
        write(g, jnp.dot(permute, stacked, preferred_element_type=F32).astype(BF16))


def unfold(wire_ref, rows_ref):
    permute = wire_permutation(True)
    part = wire_ref.shape[1]
    for g in range(wire_ref.shape[0] // 128):
        block = jnp.dot(
            permute, wire_ref[g * 128 : (g + 1) * 128, :], preferred_element_type=F32
        ).astype(BF16)
        for q in range(QUARTERS):
            rows_ref[g * 32 : (g + 1) * 32, q * part : (q + 1) * part] = block[q * 32 : (q + 1) * 32]


def project_kernel(columns_ref, heads_ref, *refs):
    pieces = refs[:8]
    residual_hbm, gain_ref, place_ref, mixed_hbm, normed_hbm, wire_ref = refs[8:14]
    weight_ref, residual_ref, part_ref, mixed_ref, normed_ref, sems = refs[14:]
    copies = [
        pltpu.make_async_copy(pieces[s], weight_ref.at[s], sems.at[s]) for s in range(8)
    ]
    copies.append(pltpu.make_async_copy(residual_hbm, residual_ref, sems.at[8]))
    copies.append(pltpu.make_async_copy(mixed_ref, mixed_hbm, sems.at[9]))
    copies.append(pltpu.make_async_copy(normed_ref, normed_hbm, sems.at[10]))
    for copy in copies[:9]:
        copy.start()
    rows = jnp.concatenate([heads_ref[h] for h in range(heads_ref.shape[0])], axis=1)
    for s in range(8):
        copies[s].wait()
        part_ref[columns_ref[s]] = jnp.dot(rows, weight_ref[s], preferred_element_type=F32)
    copies[8].wait()
    width = part_ref.shape[2]
    square = None
    for j in range(8):
        block = part_ref[j] + residual_ref[:, j * width : (j + 1) * width].astype(F32)
        mixed_ref[:, j * width : (j + 1) * width] = block
        part = jnp.sum(block * block, axis=-1, keepdims=True)
        square = part if square is None else square + part
    scale = lax.rsqrt(square * (1.0 / (8 * width)) + EPS)
    normed = (mixed_ref[...] * scale * gain_ref[...]).astype(BF16)
    normed_ref[...] = normed
    copies[9].start()
    copies[10].start()
    span = place_ref.shape[0] // PAIRS
    part = normed.shape[1] // QUARTERS
    for c in range(PAIRS):
        slots = jnp.dot(
            place_ref[c * span : (c + 1) * span, :], normed, preferred_element_type=F32
        ).astype(BF16)

        def write(g, block):
            wire_ref[g * 128 : (g + 1) * 128, c * part : (c + 1) * part] = block

        fold(slots, write)
    copies[9].wait()
    copies[10].wait()


def project(columns, heads, pieces, residual, gain, place):
    tokens, width = residual.shape
    peers = place.shape[0] // CAP
    vmem = pl.BlockSpec(memory_space=pltpu.VMEM)
    return pl.pallas_call(
        project_kernel,
        in_specs=[pl.BlockSpec(memory_space=pltpu.SMEM), vmem]
        + [pl.BlockSpec(memory_space=pl.ANY)] * 9
        + [vmem] * 2,
        out_specs=[pl.BlockSpec(memory_space=pl.ANY)] * 2 + [vmem],
        out_shape=(
            pltpu.HBM((tokens, width), F32),
            pltpu.HBM((tokens, width), BF16),
            pltpu.VMEM((peers * 8, width * CAP // 8), BF16),
        ),
        scratch_shapes=[
            pltpu.VMEM((8,) + pieces[0].shape, BF16),
            pltpu.VMEM(residual.shape, BF16),
            pltpu.VMEM((8, tokens, width // 8), F32),
            pltpu.VMEM((tokens, width), F32),
            pltpu.VMEM((tokens, width), BF16),
            pltpu.SemaphoreType.DMA((11,)),
        ],
        compiler_params=limit(32),
        name="project",
    )(
        columns,
        local(heads),
        *(distant(piece) for piece in pieces),
        distant(residual),
        gain,
        local(place),
    )


def expert_kernel(wire_ref, gate_ref, up_ref, down_ref, out_hbm, rows_ref, out_ref, sems):
    part = wire_ref.shape[1] // PAIRS
    span = rows_ref.shape[0] // PAIRS
    for c in range(PAIRS):
        unfold(
            wire_ref.at[:, pl.ds(c * part, part)], rows_ref.at[pl.ds(c * span, span)]
        )
    rows = rows_ref[...]
    gate = jnp.dot(rows, gate_ref[...], preferred_element_type=F32)
    up = jnp.dot(rows, up_ref[...], preferred_element_type=F32)
    hidden = (gate / (1.0 + jnp.exp(-gate)) * up).astype(BF16)
    copies = []
    for c in range(PAIRS):
        output = jnp.dot(
            hidden[c * span : (c + 1) * span], down_ref[...], preferred_element_type=F32
        ).astype(BF16)

        def write(g, block):
            out_ref[g * 128 : (g + 1) * 128, c * part : (c + 1) * part] = block

        fold(output, write)
        lanes = pl.ds(c * part, part)
        copies.append(
            pltpu.make_async_copy(out_ref.at[:, lanes], out_hbm.at[:, lanes], sems.at[c])
        )
        copies[c].start()
    for copy in copies:
        copy.wait()


def expert(wire, gate, up, down):
    rows, width = wire.shape
    vmem = pl.BlockSpec(memory_space=pltpu.VMEM)
    return pl.pallas_call(
        expert_kernel,
        in_specs=[vmem] * 4,
        out_specs=pl.BlockSpec(memory_space=pl.ANY),
        out_shape=pltpu.HBM(wire.shape, BF16),
        scratch_shapes=[
            pltpu.VMEM((rows * CAP // 8, width * 8 // CAP), BF16),
            pltpu.VMEM(wire.shape, BF16),
            pltpu.SemaphoreType.DMA((PAIRS,)),
        ],
        compiler_params=limit(32),
        name="expert",
    )(local(wire), local(gate), local(up), local(down))


def shared_kernel(normed_ref, mixed_ref, gate_ref, up_ref, down_ref, out_ref):
    rows = normed_ref[...]
    gate = jnp.dot(rows, gate_ref[...], preferred_element_type=F32)
    up = jnp.dot(rows, up_ref[...], preferred_element_type=F32)
    hidden = (gate / (1.0 + jnp.exp(-gate)) * up).astype(BF16)
    output = jnp.dot(hidden, down_ref[...], preferred_element_type=F32)

    @pl.when(pl.program_id(0) == 0)
    def _():
        out_ref[...] = mixed_ref[...] + output

    @pl.when(pl.program_id(0) > 0)
    def _():
        out_ref[...] = out_ref[...] + output


def shared(normed, mixed, gate, up, down):
    block = 256

    def whole(array):
        return pl.BlockSpec(array.shape, lambda i: (0, 0))

    columns = pl.BlockSpec((gate.shape[0], block), lambda i: (0, i))
    return pl.pallas_call(
        shared_kernel,
        grid=(gate.shape[1] // block,),
        in_specs=[
            whole(normed),
            whole(mixed),
            columns,
            columns,
            pl.BlockSpec((block, down.shape[1]), lambda i: (i, 0)),
        ],
        out_specs=whole(mixed),
        out_shape=pltpu.HBM(mixed.shape, F32),
        compiler_params=limit(20),
        name="shared",
    )(*(distant(array) for array in (normed, mixed, gate, up, down)))


def combine_kernel(wire_ref, gates_ref, base_hbm, out_ref, rows_ref, base_ref, sem):
    copy = pltpu.make_async_copy(base_hbm, base_ref, sem)
    copy.start()
    gates = gates_ref[...]
    tokens = gates.shape[0]
    high = gates.astype(BF16)
    rest = gates - high.astype(F32)
    middle = rest.astype(BF16)
    low = (rest - middle.astype(F32)).astype(BF16)
    stacked = jnp.concatenate([high, middle, low], axis=0)
    part = wire_ref.shape[1] // PAIRS
    span = rows_ref.shape[0] // PAIRS
    for c in range(PAIRS):
        unfold(
            wire_ref.at[:, pl.ds(c * part, part)], rows_ref.at[pl.ds(c * span, span)]
        )
    copy.wait()
    block = 512
    for n in range(base_ref.shape[1] // block):
        lanes = slice(n * block, (n + 1) * block)
        parts = jnp.dot(stacked, rows_ref[:, lanes], preferred_element_type=F32)
        routed = parts[:tokens] + (parts[tokens : 2 * tokens] + parts[2 * tokens :])
        out_ref[:, lanes] = (base_ref[:, lanes] + routed).astype(BF16)


def combine(wire, gates, base):
    rows, width = wire.shape
    vmem = pl.BlockSpec(memory_space=pltpu.VMEM)
    return pl.pallas_call(
        combine_kernel,
        in_specs=[vmem, vmem, pl.BlockSpec(memory_space=pl.ANY)],
        out_specs=vmem,
        out_shape=jax.ShapeDtypeStruct(base.shape, BF16),
        scratch_shapes=[
            pltpu.VMEM((rows * CAP // 8, width * 8 // CAP), BF16),
            pltpu.VMEM(base.shape, F32),
            pltpu.SemaphoreType.DMA,
        ],
        compiler_params=limit(24),
        name="combine",
    )(local(wire), local(gates), distant(base))


def shift(values, target):
    size = lax.axis_size("dp")

    def place(d):
        x, core = target(d // 2, d % 2)
        return 2 * (x % (size // 2)) + core

    return lax.ppermute(values, "dp", [(d, place(d)) for d in range(size)])


def apart(x, core):
    return x + 1 - 2 * core, core


def across(x, core):
    return x - 1 + 2 * core, core


def partner(x, core):
    return x, 1 - core


def per_device(
    residual,
    query,
    key_value,
    out_weight,
    norm_gain,
    query_gain,
    key_gain,
    route_ids,
    route_weights,
    shared_gate,
    shared_up,
    shared_down,
    expert_gate,
    expert_up,
    expert_down,
):
    tokens, width = residual.shape[1:]
    experts = expert_gate.shape[0] * lax.axis_size(("sp", "dp"))
    ring = lax.axis_size("dp") // 2
    blocks = lax.axis_size("sp")

    near = shift(out_weight, apart)
    other = shift(out_weight, across)
    outgoing = prepare(query[0], key_value[0], query_gain, key_gain, lax.axis_index("sp"), blocks)
    rows = lax.all_to_all(outgoing, "sp", split_axis=0, concat_axis=0, tiled=True)
    rows, near, other = lax.optimization_barrier((rows, near, other))
    far = shift(near, apart)
    attention = attend(rows.reshape(-1, rows.shape[2]))
    place, gates = route(route_ids[0], route_weights[0], experts)
    heads = lax.all_to_all(
        attention.reshape(-1, tokens, attention.shape[1]),
        "sp",
        split_axis=0,
        concat_axis=0,
        tiled=True,
    )
    own_pair, near_pair, other_pair, far_pair = [
        shift(piece, partner) for piece in (out_weight, near, other, far)
    ]

    me = lax.axis_index("dp")
    x, core = me // 2, me % 2
    away = 1 - 2 * core
    steps = jnp.array([0, 0, -1, 1, 1, -1, 2, 2], jnp.int32) * away
    flips = jnp.array([0, 1, 0, 0, 1, 1, 0, 1], jnp.int32)
    columns = 2 * ((x + steps) % ring) + (core + flips) % 2
    pieces = [out_weight, own_pair, near, other, near_pair, other_pair, far, far_pair]
    mixed, normed, wire = project(
        columns, heads, pieces, residual[0], norm_gain.reshape(1, -1), place
    )
    wire_shape = (wire.shape[0] // 8, 8, wire.shape[1])

    def exchange(values):
        return lax.all_to_all(
            values.reshape(wire_shape), ("sp", "dp"), split_axis=0, concat_axis=0, tiled=True
        ).reshape(values.shape)

    arrived = exchange(wire)
    base = shared(normed, mixed, shared_gate, shared_up, shared_down)
    output = expert(arrived, expert_gate[0], expert_up[0], expert_down[0])
    returned = exchange(output)
    return combine(returned, gates, base).reshape(1, tokens, width)


def solution(mesh):
    in_specs = (
        P("dp", "sp", None),
        P("dp", "sp", None, None),
        P("dp", "sp", None, None),
        P(None, "dp"),
        P(),
        P(),
        P(),
        P("dp", "sp", None),
        P("dp", "sp", None),
        P(),
        P(),
        P(),
        P(("sp", "dp"), None, None),
        P(("sp", "dp"), None, None),
        P(("sp", "dp"), None, None),
    )
    out_specs = P("dp", "sp", None)
    return jax.shard_map(
        per_device, mesh=mesh, in_specs=in_specs, out_specs=out_specs, check_vma=False
    )
```

```python
import jax
import jax.numpy as jnp
import numpy as np
from jax import lax
from jax.experimental import pallas as pl
from jax.experimental.pallas import tpu as pltpu
from jax.sharding import PartitionSpec as P


GRID_W = 64
HD = 64
EPS = 1e-06
THETA = 10000.0
ROUTED_SCALE = 2.5
CAP = 6
PAIRS = CAP // 2
QUARTERS = 4
F32 = jnp.float32
BF16 = jnp.bfloat16


def iota(shape, axis):
    return lax.broadcasted_iota(jnp.int32, shape, axis)


LANES = 2 * HD


def local(values):
    return pltpu.with_memory_space_constraint(values, pltpu.VMEM)


def distant(values):
    return pltpu.with_memory_space_constraint(values, pltpu.HBM)


def limit(mib):
    return pltpu.CompilerParams(vmem_limit_bytes=mib * 2**20)


def angle_tables(tokens, blocks):
    lane = np.arange(LANES)
    by_row = lane % HD < HD // 2
    freq = THETA ** (-(2.0 * (lane % (HD // 4))) / (HD // 2))
    col = (np.arange(tokens) % GRID_W)[:, None] * freq[None, :]
    row = np.arange(blocks * tokens // GRID_W)[:, None] * freq[None, :]
    col = np.where(by_row, 0.0, np.stack([np.cos(col), np.sin(col)]))
    row = np.where(by_row, np.stack([np.cos(row), np.sin(row)]), 0.0)
    row = row.reshape(2, blocks, tokens // GRID_W, LANES).transpose(1, 0, 2, 3)
    return col.astype(np.float32), row.astype(np.float32)


def prepare_kernel(
    block_ref, q_ref, kv_ref, col_ref, row_ref, q_gain_ref, k_gain_ref, out_ref, table_ref
):
    del block_ref
    tokens, heads = q_ref.shape[:2]
    shape = (tokens, LANES)
    lane = iota(shape, 1)
    is_key = lane < HD
    block = (iota((LANES, LANES), 0) // HD == iota((LANES, LANES), 1) // HD).astype(F32).astype(BF16)

    @pl.when(pl.program_id(0) == 0)
    def _():
        lower = lane % (HD // 2) < HD // 4

        def angles(which):
            rows = [
                col_ref[which, r * GRID_W : (r + 1) * GRID_W, :] + row_ref[0, which, r : r + 1, :]
                for r in range(tokens // GRID_W)
            ]
            return jnp.concatenate(rows, axis=0)

        cosine, sine = angles(0), angles(1)

        def tables(gain_ref, scale):
            gain = gain_ref[...] * scale
            gain = jnp.broadcast_to(jnp.concatenate([gain, gain], axis=1), shape)
            up = pltpu.roll(gain, LANES - HD // 4, 1)
            down = pltpu.roll(gain, HD // 4, 1)
            return (
                gain * cosine,
                jnp.where(lower, -up * sine, 0.0),
                jnp.where(lower, 0.0, down * sine),
            )

        for i, table in enumerate(tables(q_gain_ref, HD**-0.5)):
            table_ref[i] = table
        own, up, down = tables(k_gain_ref, 1.0)
        table_ref[3] = jnp.where(is_key, own, 1.0)
        table_ref[4] = jnp.where(is_key, up, 0.0)
        table_ref[5] = jnp.where(is_key, down, 0.0)

    def turned(x, base, keys):
        square = x * x
        high = square.astype(BF16)
        low = (square - high.astype(F32)).astype(BF16)
        total = jnp.dot(high, block, preferred_element_type=F32)
        total = total + jnp.dot(low, block, preferred_element_type=F32)
        scale = lax.rsqrt(total * (1.0 / HD) + EPS)
        if keys:
            scale = jnp.where(is_key, scale, 1.0)
        mixed = (
            x * table_ref[base]
            + pltpu.roll(x, LANES - HD // 4, 1) * table_ref[base + 1]
            + pltpu.roll(x, HD // 4, 1) * table_ref[base + 2]
        )
        return (mixed * scale).astype(BF16)

    query = jnp.swapaxes(q_ref[...].astype(F32), 0, 1)
    pair = jnp.swapaxes(kv_ref[...].astype(F32), 0, 1)
    for h in range(heads):
        out_ref[h, :, :LANES] = turned(query[h], 0, False)
        out_ref[h, :, LANES:] = turned(pair[h], 3, True)


def prepare(query, pair, query_gain, key_gain, block, blocks):
    tokens, heads, width = query.shape
    step = 8
    col, row = angle_tables(tokens, blocks)
    gains = [gain.reshape(1, -1) for gain in (query_gain, key_gain)]
    return pl.pallas_call(
        prepare_kernel,
        grid_spec=pltpu.PrefetchScalarGridSpec(
            num_scalar_prefetch=1,
            grid=(heads // step,),
            in_specs=[
                pl.BlockSpec((tokens, step, width), lambda i, b: (0, i, 0)),
                pl.BlockSpec((tokens, step, width), lambda i, b: (0, i, 0)),
                pl.BlockSpec(col.shape, lambda i, b: (0, 0, 0)),
                pl.BlockSpec((1,) + row.shape[1:], lambda i, b: (b[0], 0, 0, 0)),
                pl.BlockSpec((1, HD), lambda i, b: (0, 0)),
                pl.BlockSpec((1, HD), lambda i, b: (0, 0)),
            ],
            out_specs=pl.BlockSpec((step, tokens, 2 * width), lambda i, b: (i, 0, 0)),
            scratch_shapes=[pltpu.VMEM((6, tokens, width), F32)],
        ),
        out_shape=jax.ShapeDtypeStruct((heads, tokens, 2 * width), BF16),
        compiler_params=limit(16),
        name="prepare",
    )(
        jnp.full((1,), block, jnp.int32),
        *(distant(array) for array in (query, pair, jnp.asarray(col), jnp.asarray(row), *gains)),
    )


def attend_kernel(q_ref, kv_ref, out_ref, keys_ref, values_ref):
    @pl.when(pl.program_id(0) == 0)
    def _():
        key = kv_ref[:, 128 : 128 + HD]
        value = kv_ref[:, 128 + HD :]
        keys_ref[...] = jnp.concatenate([key, key], axis=1)
        values_ref[:, :128] = jnp.concatenate([value, value], axis=1)
        values_ref[:, 128:] = jnp.ones_like(values_ref[:, 128:])

    first = iota((1, 128), 1) < HD
    block = 512
    parts = [(r, head) for r in range(q_ref.shape[0] // block) for head in range(2)]

    def score(part):
        r, head = part
        query = q_ref[r * block : (r + 1) * block, :]
        mine = jnp.where(first if head == 0 else ~first, query, jnp.zeros_like(query))
        return lax.dot_general(
            mine, keys_ref[...], (((1,), (1,)), ((), ())), preferred_element_type=F32
        )

    def mix(scores):
        weights = jnp.exp(scores - jnp.max(scores, axis=-1, keepdims=True)).astype(BF16)
        mixed = jnp.dot(weights, values_ref[...], preferred_element_type=F32)
        return mixed[:, :128] / mixed[:, 128:]

    outs = []
    ahead = score(parts[0])
    for n in range(len(parts)):
        scores = ahead
        if n + 1 < len(parts):
            ahead = score(parts[n + 1])
        outs.append(mix(scores))
    for r in range(len(parts) // 2):
        out_ref[r * block : (r + 1) * block, :] = jnp.where(
            first, outs[2 * r], outs[2 * r + 1]
        ).astype(BF16)


def attend(rows):
    length, width = rows.shape
    block = 512
    return pl.pallas_call(
        attend_kernel,
        grid=(length // block,),
        in_specs=[
            pl.BlockSpec((block, 128), lambda i: (i, 0)),
            pl.BlockSpec((length, width), lambda i: (0, 0)),
        ],
        out_specs=pl.BlockSpec((block, 128), lambda i: (i, 0)),
        out_shape=pltpu.HBM((length, 128), BF16),
        scratch_shapes=[pltpu.VMEM((length, 128), BF16), pltpu.VMEM((length, 256), BF16)],
        compiler_params=limit(24),
        name="attend",
    )(rows, rows)


def route_kernel(ids_ref, weights_ref, place_ref, gates_ref):
    tokens, top = ids_ref.shape
    experts = place_ref.shape[0] // CAP
    expert = iota((tokens, experts), 1)
    hits = [(ids_ref[:, k : k + 1] == expert).astype(F32) for k in range(top)]
    used = sum(hits[1:], hits[0])
    earlier = (iota((tokens, tokens), 1) < iota((tokens, tokens), 0)).astype(F32).astype(BF16)
    before = jnp.dot(earlier, used.astype(BF16), preferred_element_type=F32)
    raw = weights_ref[...]
    gate = raw / jnp.sum(raw, axis=-1, keepdims=True) * ROUTED_SCALE
    slots = iota((tokens, experts * CAP), 1)
    place = jnp.zeros((tokens, experts * CAP), F32)
    gated = jnp.zeros((tokens, experts * CAP), F32)
    for k in range(top):
        rank = jnp.sum(hits[k] * before, axis=-1, keepdims=True).astype(jnp.int32)
        slot = (rank // 2) * (2 * experts) + ids_ref[:, k : k + 1] * 2 + rank % 2
        here = slots == slot
        place = jnp.where(here, 1.0, place)
        gated = jnp.where(here, gate[:, k : k + 1], gated)
    place_ref[...] = jnp.transpose(place).astype(BF16)
    gates_ref[...] = gated


def route(ids, weights, experts):
    tokens, _ = ids.shape
    return pl.pallas_call(
        route_kernel,
        out_shape=(
            pltpu.VMEM((experts * CAP, tokens), BF16),
            pltpu.VMEM((tokens, experts * CAP), F32),
        ),
        compiler_params=limit(8),
        name="route",
    )(ids, weights)


def wire_permutation(transposed):
    wire = iota((128, 128), 1 if transposed else 0)
    flat = iota((128, 128), 0 if transposed else 1)
    source = (wire // 2 % QUARTERS) * 32 + (wire // 8) * 2 + wire % 2
    return (flat == source).astype(F32).astype(BF16)


def fold(rows, write):
    permute = wire_permutation(False)
    part = rows.shape[1] // QUARTERS
    for g in range(rows.shape[0] // 32):
        stacked = jnp.concatenate(
            [rows[g * 32 : (g + 1) * 32, q * part : (q + 1) * part] for q in range(QUARTERS)], axis=0
        )
        write(g, jnp.dot(permute, stacked, preferred_element_type=F32).astype(BF16))


def unfold(wire_ref, rows_ref):
    permute = wire_permutation(True)
    part = wire_ref.shape[1]
    for g in range(wire_ref.shape[0] // 128):
        block = jnp.dot(
            permute, wire_ref[g * 128 : (g + 1) * 128, :], preferred_element_type=F32
        ).astype(BF16)
        for q in range(QUARTERS):
            rows_ref[g * 32 : (g + 1) * 32, q * part : (q + 1) * part] = block[q * 32 : (q + 1) * 32]


def project_kernel(columns_ref, heads_ref, *refs):
    placed, pieces = refs[:2], refs[2:8]
    residual_hbm, gain_ref, place_ref, mixed_hbm, normed_hbm, wire_ref = refs[8:14]
    weight_ref, residual_ref, part_ref, mixed_ref, normed_ref, sems = refs[14:]
    copies = [
        pltpu.make_async_copy(pieces[s], weight_ref.at[s], sems.at[s]) for s in range(6)
    ]
    copies.append(pltpu.make_async_copy(residual_hbm, residual_ref, sems.at[6]))
    copies.append(pltpu.make_async_copy(mixed_ref, mixed_hbm, sems.at[7]))
    copies.append(pltpu.make_async_copy(normed_ref, normed_hbm, sems.at[8]))
    for copy in copies[:7]:
        copy.start()
    rows = jnp.concatenate([heads_ref[h] for h in range(heads_ref.shape[0])], axis=1)
    for s in range(8):
        if s >= 2:
            copies[s - 2].wait()
        weight = weight_ref[s - 2] if s >= 2 else placed[s][...]
        part_ref[columns_ref[s]] = jnp.dot(rows, weight, preferred_element_type=F32)
    copies[6].wait()
    width = part_ref.shape[2]
    square = None
    for j in range(8):
        block = part_ref[j] + residual_ref[:, j * width : (j + 1) * width].astype(F32)
        mixed_ref[:, j * width : (j + 1) * width] = block
        part = jnp.sum(block * block, axis=-1, keepdims=True)
        square = part if square is None else square + part
    scale = lax.rsqrt(square * (1.0 / (8 * width)) + EPS)
    normed = (mixed_ref[...] * scale * gain_ref[...]).astype(BF16)
    normed_ref[...] = normed
    copies[7].start()
    copies[8].start()
    span = place_ref.shape[0] // PAIRS
    part = normed.shape[1] // QUARTERS
    for c in range(PAIRS):
        slots = jnp.dot(
            place_ref[c * span : (c + 1) * span, :], normed, preferred_element_type=F32
        ).astype(BF16)

        def write(g, block):
            wire_ref[g * 128 : (g + 1) * 128, c * part : (c + 1) * part] = block

        fold(slots, write)
    copies[7].wait()
    copies[8].wait()


def project(columns, heads, pieces, residual, gain, place):
    tokens, width = residual.shape
    peers = place.shape[0] // CAP
    vmem = pl.BlockSpec(memory_space=pltpu.VMEM)
    return pl.pallas_call(
        project_kernel,
        in_specs=[pl.BlockSpec(memory_space=pltpu.SMEM)]
        + [vmem] * 3
        + [pl.BlockSpec(memory_space=pl.ANY)] * 7
        + [vmem] * 2,
        out_specs=[pl.BlockSpec(memory_space=pl.ANY)] * 2 + [vmem],
        out_shape=(
            pltpu.HBM((tokens, width), F32),
            pltpu.HBM((tokens, width), BF16),
            pltpu.VMEM((peers * 8, width * CAP // 8), BF16),
        ),
        scratch_shapes=[
            pltpu.VMEM((6,) + pieces[0].shape, BF16),
            pltpu.VMEM(residual.shape, BF16),
            pltpu.VMEM((8, tokens, width // 8), F32),
            pltpu.VMEM((tokens, width), F32),
            pltpu.VMEM((tokens, width), BF16),
            pltpu.SemaphoreType.DMA((9,)),
        ],
        compiler_params=limit(24),
        name="project",
    )(
        columns,
        local(heads),
        *(local(piece) for piece in pieces[:2]),
        *(distant(piece) for piece in pieces[2:]),
        distant(residual),
        gain,
        local(place),
    )


def expert_kernel(wire_ref, gate_ref, up_ref, down_ref, out_hbm, rows_ref, out_ref, sems):
    part = wire_ref.shape[1] // PAIRS
    span = rows_ref.shape[0] // PAIRS
    for c in range(PAIRS):
        unfold(
            wire_ref.at[:, pl.ds(c * part, part)], rows_ref.at[pl.ds(c * span, span)]
        )
    rows = rows_ref[...]
    gate = jnp.dot(rows, gate_ref[...], preferred_element_type=F32)
    up = jnp.dot(rows, up_ref[...], preferred_element_type=F32)
    hidden = (gate / (1.0 + jnp.exp(-gate)) * up).astype(BF16)
    copies = []
    for c in range(PAIRS):
        output = jnp.dot(
            hidden[c * span : (c + 1) * span], down_ref[...], preferred_element_type=F32
        ).astype(BF16)

        def write(g, block):
            out_ref[g * 128 : (g + 1) * 128, c * part : (c + 1) * part] = block

        fold(output, write)
        lanes = pl.ds(c * part, part)
        copies.append(
            pltpu.make_async_copy(out_ref.at[:, lanes], out_hbm.at[:, lanes], sems.at[c])
        )
        copies[c].start()
    for copy in copies:
        copy.wait()


def expert(wire, gate, up, down):
    rows, width = wire.shape
    vmem = pl.BlockSpec(memory_space=pltpu.VMEM)
    return pl.pallas_call(
        expert_kernel,
        in_specs=[vmem] * 4,
        out_specs=pl.BlockSpec(memory_space=pl.ANY),
        out_shape=pltpu.HBM(wire.shape, BF16),
        scratch_shapes=[
            pltpu.VMEM((rows * CAP // 8, width * 8 // CAP), BF16),
            pltpu.VMEM(wire.shape, BF16),
            pltpu.SemaphoreType.DMA((PAIRS,)),
        ],
        compiler_params=limit(32),
        name="expert",
    )(local(wire), local(gate), local(up), local(down))


def shared_kernel(normed_ref, mixed_ref, gate_ref, up_ref, down_ref, out_ref):
    rows = normed_ref[...]
    gate = jnp.dot(rows, gate_ref[...], preferred_element_type=F32)
    up = jnp.dot(rows, up_ref[...], preferred_element_type=F32)
    hidden = (gate / (1.0 + jnp.exp(-gate)) * up).astype(BF16)
    output = jnp.dot(hidden, down_ref[...], preferred_element_type=F32)

    @pl.when(pl.program_id(0) == 0)
    def _():
        out_ref[...] = mixed_ref[...] + output

    @pl.when(pl.program_id(0) > 0)
    def _():
        out_ref[...] = out_ref[...] + output


def shared(normed, mixed, gate, up, down):
    block = 256

    def whole(array):
        return pl.BlockSpec(array.shape, lambda i: (0, 0))

    columns = pl.BlockSpec((gate.shape[0], block), lambda i: (0, i))
    return pl.pallas_call(
        shared_kernel,
        grid=(gate.shape[1] // block,),
        in_specs=[
            whole(normed),
            whole(mixed),
            columns,
            columns,
            pl.BlockSpec((block, down.shape[1]), lambda i: (i, 0)),
        ],
        out_specs=whole(mixed),
        out_shape=pltpu.HBM(mixed.shape, F32),
        compiler_params=limit(20),
        name="shared",
    )(*(distant(array) for array in (normed, mixed, gate, up, down)))


def combine_kernel(wire_ref, gates_ref, base_hbm, out_hbm, rows_ref, base_ref, out_ref, sems):
    blocks = sems.shape[0] - 1
    block = base_ref.shape[1] // blocks
    fetch = pltpu.make_async_copy(base_hbm, base_ref, sems.at[blocks])
    fetch.start()
    gates = gates_ref[...]
    tokens = gates.shape[0]
    high = gates.astype(BF16)
    low = (gates - high.astype(F32)).astype(BF16)
    stacked = jnp.concatenate([high, low], axis=0)
    part = wire_ref.shape[1] // PAIRS
    span = rows_ref.shape[0] // PAIRS
    for c in range(PAIRS):
        unfold(
            wire_ref.at[:, pl.ds(c * part, part)], rows_ref.at[pl.ds(c * span, span)]
        )
    fetch.wait()
    copies = []
    for n in range(blocks):
        lanes = slice(n * block, (n + 1) * block)
        parts = jnp.dot(stacked, rows_ref[:, lanes], preferred_element_type=F32)
        routed = parts[:tokens] + parts[tokens:]
        out_ref[:, lanes] = (base_ref[:, lanes] + routed).astype(BF16)
        lanes = pl.ds(n * block, block)
        copies.append(
            pltpu.make_async_copy(out_ref.at[:, lanes], out_hbm.at[:, lanes], sems.at[n])
        )
        copies[n].start()
    for copy in copies:
        copy.wait()


def combine(wire, gates, base):
    rows, width = wire.shape
    vmem = pl.BlockSpec(memory_space=pltpu.VMEM)
    return pl.pallas_call(
        combine_kernel,
        in_specs=[vmem, vmem, pl.BlockSpec(memory_space=pl.ANY)],
        out_specs=pl.BlockSpec(memory_space=pl.ANY),
        out_shape=pltpu.HBM(base.shape, BF16),
        scratch_shapes=[
            pltpu.VMEM((rows * CAP // 8, width * 8 // CAP), BF16),
            pltpu.VMEM(base.shape, F32),
            pltpu.VMEM(base.shape, BF16),
            pltpu.SemaphoreType.DMA((5,)),
        ],
        compiler_params=limit(24),
        name="combine",
    )(local(wire), local(gates), distant(base))


def shift(values, target):
    size = lax.axis_size("dp")

    def place(d):
        x, core = target(d // 2, d % 2)
        return 2 * (x % (size // 2)) + core

    return lax.ppermute(values, "dp", [(d, place(d)) for d in range(size)])


def apart(x, core):
    return x + 1 - 2 * core, core


def across(x, core):
    return x - 1 + 2 * core, core


def partner(x, core):
    return x, 1 - core


def per_device(
    residual,
    query,
    key_value,
    out_weight,
    norm_gain,
    query_gain,
    key_gain,
    route_ids,
    route_weights,
    shared_gate,
    shared_up,
    shared_down,
    expert_gate,
    expert_up,
    expert_down,
):
    tokens, width = residual.shape[1:]
    experts = expert_gate.shape[0] * lax.axis_size(("sp", "dp"))
    ring = lax.axis_size("dp") // 2
    blocks = lax.axis_size("sp")

    near = shift(out_weight, apart)
    other = shift(out_weight, across)
    outgoing = prepare(query[0], key_value[0], query_gain, key_gain, lax.axis_index("sp"), blocks)
    rows = lax.all_to_all(outgoing, "sp", split_axis=0, concat_axis=0, tiled=True)
    rows, near, other = lax.optimization_barrier((rows, near, other))
    far = shift(near, apart)
    attention = attend(rows.reshape(-1, rows.shape[2]))
    place, gates = route(route_ids[0], route_weights[0], experts)
    heads = lax.all_to_all(
        attention.reshape(-1, tokens, attention.shape[1]),
        "sp",
        split_axis=0,
        concat_axis=0,
        tiled=True,
    )
    own_pair, near_pair, other_pair, far_pair = [
        shift(piece, partner) for piece in (out_weight, near, other, far)
    ]

    me = lax.axis_index("dp")
    x, core = me // 2, me % 2
    away = 1 - 2 * core
    steps = jnp.array([0, 1, -1, 0, 1, -1, 2, 2], jnp.int32) * away
    flips = jnp.array([0, 0, 0, 1, 1, 1, 0, 1], jnp.int32)
    columns = 2 * ((x + steps) % ring) + (core + flips) % 2
    pieces = [out_weight, other, near, own_pair, near_pair, other_pair, far, far_pair]
    mixed, normed, wire = project(
        columns, heads, pieces, residual[0], norm_gain.reshape(1, -1), place
    )
    wire_shape = (wire.shape[0] // 8, 8, wire.shape[1])

    def exchange(values):
        return lax.all_to_all(
            values.reshape(wire_shape), ("sp", "dp"), split_axis=0, concat_axis=0, tiled=True
        ).reshape(values.shape)

    arrived = exchange(wire)
    base = shared(normed, mixed, shared_gate, shared_up, shared_down)
    output = expert(arrived, expert_gate[0], expert_up[0], expert_down[0])
    returned = exchange(output)
    return combine(returned, gates, base).reshape(1, tokens, width)


def solution(mesh):
    in_specs = (
        P("dp", "sp", None),
        P("dp", "sp", None, None),
        P("dp", "sp", None, None),
        P(None, "dp"),
        P(),
        P(),
        P(),
        P("dp", "sp", None),
        P("dp", "sp", None),
        P(),
        P(),
        P(),
        P(("sp", "dp"), None, None),
        P(("sp", "dp"), None, None),
        P(("sp", "dp"), None, None),
    )
    out_specs = P("dp", "sp", None)
    return jax.shard_map(
        per_device, mesh=mesh, in_specs=in_specs, out_specs=out_specs, check_vma=False
    )
```

```python
import jax
import jax.numpy as jnp
import numpy as np
from jax import lax
from jax.experimental import pallas as pl
from jax.experimental.pallas import tpu as pltpu
from jax.sharding import PartitionSpec as P


GRID_W = 64
HD = 64
EPS = 1e-06
THETA = 10000.0
ROUTED_SCALE = 2.5
CAP = 6
PAIRS = CAP // 2
F32 = jnp.float32
BF16 = jnp.bfloat16


def iota(shape, axis):
    return lax.broadcasted_iota(jnp.int32, shape, axis)


LANES = 2 * HD


def local(values):
    return pltpu.with_memory_space_constraint(values, pltpu.VMEM)


def distant(values):
    return pltpu.with_memory_space_constraint(values, pltpu.HBM)


def limit(mib):
    return pltpu.CompilerParams(vmem_limit_bytes=mib * 2**20)


def angle_tables(tokens, blocks):
    lane = np.arange(LANES)
    by_row = lane % HD < HD // 2
    freq = THETA ** (-(2.0 * (lane % (HD // 4))) / (HD // 2))
    col = (np.arange(tokens) % GRID_W)[:, None] * freq[None, :]
    row = np.arange(blocks * tokens // GRID_W)[:, None] * freq[None, :]
    col = np.where(by_row, 0.0, np.stack([np.cos(col), np.sin(col)]))
    row = np.where(by_row, np.stack([np.cos(row), np.sin(row)]), 0.0)
    row = row.reshape(2, blocks, tokens // GRID_W, LANES).transpose(1, 0, 2, 3)
    return col.astype(np.float32), row.astype(np.float32)


def prepare_kernel(
    block_ref, q_ref, kv_ref, col_ref, row_ref, q_gain_ref, k_gain_ref, out_ref, table_ref
):
    del block_ref
    tokens, heads = q_ref.shape[:2]
    shape = (tokens, LANES)
    lane = iota(shape, 1)
    is_key = lane < HD
    block = (iota((LANES, LANES), 0) // HD == iota((LANES, LANES), 1) // HD).astype(F32).astype(BF16)

    @pl.when(pl.program_id(0) == 0)
    def _():
        lower = lane % (HD // 2) < HD // 4

        def angles(which):
            rows = [
                col_ref[which, r * GRID_W : (r + 1) * GRID_W, :] + row_ref[0, which, r : r + 1, :]
                for r in range(tokens // GRID_W)
            ]
            return jnp.concatenate(rows, axis=0)

        cosine, sine = angles(0), angles(1)

        def tables(gain_ref, scale):
            gain = gain_ref[...] * scale
            gain = jnp.broadcast_to(jnp.concatenate([gain, gain], axis=1), shape)
            up = pltpu.roll(gain, LANES - HD // 4, 1)
            down = pltpu.roll(gain, HD // 4, 1)
            return (
                gain * cosine,
                jnp.where(lower, -up * sine, 0.0),
                jnp.where(lower, 0.0, down * sine),
            )

        for i, table in enumerate(tables(q_gain_ref, HD**-0.5)):
            table_ref[i] = table
        own, up, down = tables(k_gain_ref, 1.0)
        table_ref[3] = jnp.where(is_key, own, 1.0)
        table_ref[4] = jnp.where(is_key, up, 0.0)
        table_ref[5] = jnp.where(is_key, down, 0.0)

    def turned(x, base, keys):
        square = x * x
        high = square.astype(BF16)
        low = (square - high.astype(F32)).astype(BF16)
        total = jnp.dot(high, block, preferred_element_type=F32)
        total = total + jnp.dot(low, block, preferred_element_type=F32)
        scale = lax.rsqrt(total * (1.0 / HD) + EPS)
        if keys:
            scale = jnp.where(is_key, scale, 1.0)
        mixed = (
            x * table_ref[base]
            + pltpu.roll(x, LANES - HD // 4, 1) * table_ref[base + 1]
            + pltpu.roll(x, HD // 4, 1) * table_ref[base + 2]
        )
        return (mixed * scale).astype(BF16)

    query = jnp.swapaxes(q_ref[...].astype(F32), 0, 1)
    pair = jnp.swapaxes(kv_ref[...].astype(F32), 0, 1)
    for h in range(heads):
        out_ref[h, :, :LANES] = turned(query[h], 0, False)
        out_ref[h, :, LANES:] = turned(pair[h], 3, True)


def prepare(query, pair, query_gain, key_gain, block, blocks):
    tokens, heads, width = query.shape
    step = 8
    col, row = angle_tables(tokens, blocks)
    gains = [gain.reshape(1, -1) for gain in (query_gain, key_gain)]
    return pl.pallas_call(
        prepare_kernel,
        grid_spec=pltpu.PrefetchScalarGridSpec(
            num_scalar_prefetch=1,
            grid=(heads // step,),
            in_specs=[
                pl.BlockSpec((tokens, step, width), lambda i, b: (0, i, 0)),
                pl.BlockSpec((tokens, step, width), lambda i, b: (0, i, 0)),
                pl.BlockSpec(col.shape, lambda i, b: (0, 0, 0)),
                pl.BlockSpec((1,) + row.shape[1:], lambda i, b: (b[0], 0, 0, 0)),
                pl.BlockSpec((1, HD), lambda i, b: (0, 0)),
                pl.BlockSpec((1, HD), lambda i, b: (0, 0)),
            ],
            out_specs=pl.BlockSpec((step, tokens, 2 * width), lambda i, b: (i, 0, 0)),
            scratch_shapes=[pltpu.VMEM((6, tokens, width), F32)],
        ),
        out_shape=jax.ShapeDtypeStruct((heads, tokens, 2 * width), BF16),
        compiler_params=limit(16),
        name="prepare",
    )(
        jnp.full((1,), block, jnp.int32),
        *(distant(array) for array in (query, pair, jnp.asarray(col), jnp.asarray(row), *gains)),
    )


def attend_kernel(q_ref, kv_ref, out_ref, keys_ref, values_ref):
    @pl.when(pl.program_id(0) == 0)
    def _():
        key = kv_ref[:, 128 : 128 + HD]
        value = kv_ref[:, 128 + HD :]
        keys_ref[...] = jnp.concatenate([key, key], axis=1)
        values_ref[:, :128] = jnp.concatenate([value, value], axis=1)
        values_ref[:, 128:] = jnp.ones_like(values_ref[:, 128:])

    first = iota((1, 128), 1) < HD
    block = 512
    parts = [(r, head) for r in range(q_ref.shape[0] // block) for head in range(2)]

    def score(part):
        r, head = part
        query = q_ref[r * block : (r + 1) * block, :]
        mine = jnp.where(first if head == 0 else ~first, query, jnp.zeros_like(query))
        return lax.dot_general(
            mine, keys_ref[...], (((1,), (1,)), ((), ())), preferred_element_type=F32
        )

    def mix(scores):
        weights = jnp.exp(scores - jnp.max(scores, axis=-1, keepdims=True)).astype(BF16)
        mixed = jnp.dot(weights, values_ref[...], preferred_element_type=F32)
        return mixed[:, :128] / mixed[:, 128:]

    outs = []
    ahead = score(parts[0])
    for n in range(len(parts)):
        scores = ahead
        if n + 1 < len(parts):
            ahead = score(parts[n + 1])
        outs.append(mix(scores))
    for r in range(len(parts) // 2):
        out_ref[r * block : (r + 1) * block, :] = jnp.where(
            first, outs[2 * r], outs[2 * r + 1]
        ).astype(BF16)


def attend(rows):
    length, width = rows.shape
    block = 512
    return pl.pallas_call(
        attend_kernel,
        grid=(length // block,),
        in_specs=[
            pl.BlockSpec((block, 128), lambda i: (i, 0)),
            pl.BlockSpec((length, width), lambda i: (0, 0)),
        ],
        out_specs=pl.BlockSpec((block, 128), lambda i: (i, 0)),
        out_shape=pltpu.HBM((length, 128), BF16),
        scratch_shapes=[pltpu.VMEM((length, 128), BF16), pltpu.VMEM((length, 256), BF16)],
        compiler_params=limit(24),
        name="attend",
    )(rows, rows)


def route_kernel(ids_ref, weights_ref, place_ref, gates_ref):
    tokens, top = ids_ref.shape
    experts = place_ref.shape[0] // CAP
    expert = iota((tokens, experts), 1)
    hits = [(ids_ref[:, k : k + 1] == expert).astype(F32) for k in range(top)]
    used = sum(hits[1:], hits[0])
    earlier = (iota((tokens, tokens), 1) < iota((tokens, tokens), 0)).astype(F32).astype(BF16)
    before = jnp.dot(earlier, used.astype(BF16), preferred_element_type=F32)
    raw = weights_ref[...]
    gate = raw / jnp.sum(raw, axis=-1, keepdims=True) * ROUTED_SCALE
    slots = iota((tokens, experts * CAP), 1)
    place = jnp.zeros((tokens, experts * CAP), F32)
    gated = jnp.zeros((tokens, experts * CAP), F32)
    for k in range(top):
        rank = jnp.sum(hits[k] * before, axis=-1, keepdims=True).astype(jnp.int32)
        slot = rank * experts + ids_ref[:, k : k + 1]
        here = slots == slot
        place = jnp.where(here, 1.0, place)
        gated = jnp.where(here, gate[:, k : k + 1], gated)
    place_ref[...] = jnp.transpose(place).astype(BF16)
    gates_ref[...] = gated


def route(ids, weights, experts):
    tokens, _ = ids.shape
    return pl.pallas_call(
        route_kernel,
        out_shape=(
            pltpu.VMEM((experts * CAP, tokens), BF16),
            pltpu.VMEM((tokens, experts * CAP), F32),
        ),
        compiler_params=limit(8),
        name="route",
    )(ids, weights)


CHUNKS = 8


def fold(rows, wire_ref, slot):
    peers, width = rows.shape
    for half in range(width // (CHUNKS * 128)):
        first = half * CHUNKS * 128
        chunks = jnp.stack(
            [rows[:, first + n * 128 : first + (n + 1) * 128] for n in range(CHUNKS)]
        )
        block = jnp.swapaxes(chunks, 0, 1).reshape(peers * CHUNKS, 128)
        lane = (slot * (width // (CHUNKS * 128)) + half) * 128
        wire_ref[:, lane : lane + 128] = block.astype(BF16)


def unfold(wire_ref, rows_ref):
    group = 128 // CHUNKS
    peers = wire_ref.shape[0] // CHUNKS
    halves = rows_ref.shape[1] // (CHUNKS * 128)
    sent, kept = iota((128, 128), 1), iota((128, 128), 0)
    permute = (sent == kept % group * CHUNKS + kept // group).astype(F32).astype(BF16)
    for g in range(peers // group):
        block = jnp.dot(
            permute, wire_ref[g * 128 : (g + 1) * 128, :], preferred_element_type=F32
        ).astype(BF16)
        for slot in range(CAP):
            first = slot * peers + g * group
            for chunk in range(halves * CHUNKS):
                lane = (slot * halves + chunk // CHUNKS) * 128
                row = chunk % CHUNKS * group
                rows_ref[first : first + group, chunk * 128 : (chunk + 1) * 128] = block[
                    row : row + group, lane : lane + 128
                ]


def unfold_slots(wire_ref, rows_ref, slots):
    peers = wire_ref.shape[0] // CHUNKS
    halves = rows_ref.shape[1] // (CHUNKS * 128)
    for slot in slots:
        for half in range(halves):
            lane = (slot * halves + half) * 128
            block = wire_ref[:, lane : lane + 128].astype(F32).reshape(peers, CHUNKS, 128)
            chunks = jnp.swapaxes(block, 0, 1).astype(BF16)
            for n in range(CHUNKS):
                at = (half * CHUNKS + n) * 128
                rows_ref[slot * peers : (slot + 1) * peers, at : at + 128] = chunks[n]


def project_kernel(columns_ref, heads_ref, *refs):
    placed, pieces = refs[:2], refs[2:8]
    residual_hbm, gain_ref, place_ref, mixed_hbm, normed_hbm, wire_ref = refs[8:14]
    weight_ref, residual_ref, part_ref, mixed_ref, normed_ref, sems = refs[14:]
    copies = [
        pltpu.make_async_copy(pieces[s], weight_ref.at[s], sems.at[s]) for s in range(6)
    ]
    copies.append(pltpu.make_async_copy(residual_hbm, residual_ref, sems.at[6]))
    copies.append(pltpu.make_async_copy(mixed_ref, mixed_hbm, sems.at[7]))
    copies.append(pltpu.make_async_copy(normed_ref, normed_hbm, sems.at[8]))
    for copy in copies[:7]:
        copy.start()
    rows = jnp.concatenate([heads_ref[h] for h in range(heads_ref.shape[0])], axis=1)
    for s in range(8):
        if s >= 2:
            copies[s - 2].wait()
        weight = weight_ref[s - 2] if s >= 2 else placed[s][...]
        part_ref[columns_ref[s]] = jnp.dot(rows, weight, preferred_element_type=F32)
    copies[6].wait()
    width = part_ref.shape[2]
    square = None
    for j in range(8):
        block = part_ref[j] + residual_ref[:, j * width : (j + 1) * width].astype(F32)
        mixed_ref[:, j * width : (j + 1) * width] = block
        part = jnp.sum(block * block, axis=-1, keepdims=True)
        square = part if square is None else square + part
    scale = lax.rsqrt(square * (1.0 / (8 * width)) + EPS)
    normed = (mixed_ref[...] * scale * gain_ref[...]).astype(BF16)
    normed_ref[...] = normed
    copies[7].start()
    copies[8].start()
    peers = place_ref.shape[0] // CAP
    for slot in range(CAP):
        rows = jnp.dot(
            place_ref[slot * peers : (slot + 1) * peers, :], normed, preferred_element_type=F32
        )
        fold(rows, wire_ref, slot)
    copies[7].wait()
    copies[8].wait()


def project(columns, heads, pieces, residual, gain, place):
    tokens, width = residual.shape
    peers = place.shape[0] // CAP
    vmem = pl.BlockSpec(memory_space=pltpu.VMEM)
    return pl.pallas_call(
        project_kernel,
        in_specs=[pl.BlockSpec(memory_space=pltpu.SMEM)]
        + [vmem] * 3
        + [pl.BlockSpec(memory_space=pl.ANY)] * 7
        + [vmem] * 2,
        out_specs=[pl.BlockSpec(memory_space=pl.ANY)] * 2 + [vmem],
        out_shape=(
            pltpu.HBM((tokens, width), F32),
            pltpu.HBM((tokens, width), BF16),
            pltpu.VMEM((peers * 8, width * CAP // 8), BF16),
        ),
        scratch_shapes=[
            pltpu.VMEM((6,) + pieces[0].shape, BF16),
            pltpu.VMEM(residual.shape, BF16),
            pltpu.VMEM((8, tokens, width // 8), F32),
            pltpu.VMEM((tokens, width), F32),
            pltpu.VMEM((tokens, width), BF16),
            pltpu.SemaphoreType.DMA((9,)),
        ],
        compiler_params=limit(24),
        name="project",
    )(
        columns,
        local(heads),
        *(local(piece) for piece in pieces[:2]),
        *(distant(piece) for piece in pieces[2:]),
        distant(residual),
        gain,
        local(place),
    )


def expert_kernel(wire_ref, gate_ref, up_ref, down_ref, out_hbm, rows_ref, out_ref, sems):
    peers = rows_ref.shape[0] // CAP
    part = out_ref.shape[1] // PAIRS
    copies = []

    def finish(c, output):
        fold(output[:peers], out_ref, 2 * c)
        fold(output[peers:], out_ref, 2 * c + 1)
        lanes = pl.ds(c * part, part)
        copies.append(
            pltpu.make_async_copy(out_ref.at[:, lanes], out_hbm.at[:, lanes], sems.at[c])
        )
        copies[c].start()

    def hidden_of(rows):
        gate = jnp.dot(rows, gate_ref[...], preferred_element_type=F32)
        up = jnp.dot(rows, up_ref[...], preferred_element_type=F32)
        return (gate / (1.0 + jnp.exp(-gate)) * up).astype(BF16)

    def output_of(hidden):
        return jnp.dot(hidden, down_ref[...], preferred_element_type=F32)

    unfold_slots(wire_ref, rows_ref, range(CAP))
    hidden = hidden_of(rows_ref[...])
    for c in range(PAIRS):
        finish(c, output_of(hidden[c * 2 * peers : (c + 1) * 2 * peers]))
    for copy in copies:
        copy.wait()


def expert(wire, gate, up, down):
    rows, width = wire.shape
    vmem = pl.BlockSpec(memory_space=pltpu.VMEM)
    return pl.pallas_call(
        expert_kernel,
        in_specs=[vmem] * 4,
        out_specs=pl.BlockSpec(memory_space=pl.ANY),
        out_shape=pltpu.HBM(wire.shape, BF16),
        scratch_shapes=[
            pltpu.VMEM((rows * CAP // 8, width * 8 // CAP), BF16),
            pltpu.VMEM(wire.shape, BF16),
            pltpu.SemaphoreType.DMA((PAIRS,)),
        ],
        compiler_params=limit(32),
        name="expert",
    )(local(wire), local(gate), local(up), local(down))


def shared_kernel(normed_ref, mixed_ref, gate_ref, up_ref, down_ref, out_ref):
    rows = normed_ref[...]
    gate = jnp.dot(rows, gate_ref[...], preferred_element_type=F32)
    up = jnp.dot(rows, up_ref[...], preferred_element_type=F32)
    hidden = (gate / (1.0 + jnp.exp(-gate)) * up).astype(BF16)
    output = jnp.dot(hidden, down_ref[...], preferred_element_type=F32)

    @pl.when(pl.program_id(0) == 0)
    def _():
        out_ref[...] = mixed_ref[...] + output

    @pl.when(pl.program_id(0) > 0)
    def _():
        out_ref[...] = out_ref[...] + output


def shared(normed, mixed, gate, up, down):
    block = 256

    def whole(array):
        return pl.BlockSpec(array.shape, lambda i: (0, 0))

    columns = pl.BlockSpec((gate.shape[0], block), lambda i: (0, i))
    return pl.pallas_call(
        shared_kernel,
        grid=(gate.shape[1] // block,),
        in_specs=[
            whole(normed),
            whole(mixed),
            columns,
            columns,
            pl.BlockSpec((block, down.shape[1]), lambda i: (i, 0)),
        ],
        out_specs=whole(mixed),
        out_shape=pltpu.HBM(mixed.shape, F32),
        compiler_params=limit(20),
        name="shared",
    )(*(distant(array) for array in (normed, mixed, gate, up, down)))


def combine_kernel(wire_ref, gates_ref, base_hbm, out_hbm, rows_ref, base_ref, out_ref, sems):
    blocks = sems.shape[0] - 1
    block = base_ref.shape[1] // blocks
    fetch = pltpu.make_async_copy(base_hbm, base_ref, sems.at[blocks])
    fetch.start()
    gates = gates_ref[...]
    tokens = gates.shape[0]
    high = gates.astype(BF16)
    low = (gates - high.astype(F32)).astype(BF16)
    stacked = jnp.concatenate([high, low], axis=0)
    unfold(wire_ref, rows_ref)
    fetch.wait()
    copies = []
    for n in range(blocks):
        lanes = slice(n * block, (n + 1) * block)
        parts = jnp.dot(stacked, rows_ref[:, lanes], preferred_element_type=F32)
        routed = parts[:tokens] + parts[tokens:]
        out_ref[:, lanes] = (base_ref[:, lanes] + routed).astype(BF16)
        lanes = pl.ds(n * block, block)
        copies.append(
            pltpu.make_async_copy(out_ref.at[:, lanes], out_hbm.at[:, lanes], sems.at[n])
        )
        copies[n].start()
    for copy in copies:
        copy.wait()


def combine(wire, gates, base):
    rows, width = wire.shape
    vmem = pl.BlockSpec(memory_space=pltpu.VMEM)
    return pl.pallas_call(
        combine_kernel,
        in_specs=[vmem, vmem, pl.BlockSpec(memory_space=pl.ANY)],
        out_specs=pl.BlockSpec(memory_space=pl.ANY),
        out_shape=pltpu.HBM(base.shape, BF16),
        scratch_shapes=[
            pltpu.VMEM((rows * CAP // 8, width * 8 // CAP), BF16),
            pltpu.VMEM(base.shape, F32),
            pltpu.VMEM(base.shape, BF16),
            pltpu.SemaphoreType.DMA((5,)),
        ],
        compiler_params=limit(24),
        name="combine",
    )(local(wire), local(gates), distant(base))


def shift(values, target):
    size = lax.axis_size("dp")

    def place(d):
        x, core = target(d // 2, d % 2)
        return 2 * (x % (size // 2)) + core

    return lax.ppermute(values, "dp", [(d, place(d)) for d in range(size)])


def apart(x, core):
    return x + 1 - 2 * core, core


def across(x, core):
    return x - 1 + 2 * core, core


def partner(x, core):
    return x, 1 - core


def per_device(
    residual,
    query,
    key_value,
    out_weight,
    norm_gain,
    query_gain,
    key_gain,
    route_ids,
    route_weights,
    shared_gate,
    shared_up,
    shared_down,
    expert_gate,
    expert_up,
    expert_down,
):
    tokens, width = residual.shape[1:]
    experts = expert_gate.shape[0] * lax.axis_size(("sp", "dp"))
    ring = lax.axis_size("dp") // 2
    blocks = lax.axis_size("sp")

    near = shift(out_weight, apart)
    other = shift(out_weight, across)
    outgoing = prepare(query[0], key_value[0], query_gain, key_gain, lax.axis_index("sp"), blocks)
    rows = lax.all_to_all(outgoing, "sp", split_axis=0, concat_axis=0, tiled=True)
    rows, near, other = lax.optimization_barrier((rows, near, other))
    far = shift(near, apart)
    attention = attend(rows.reshape(-1, rows.shape[2]))
    place, gates = route(route_ids[0], route_weights[0], experts)
    heads = lax.all_to_all(
        attention.reshape(-1, tokens, attention.shape[1]),
        "sp",
        split_axis=0,
        concat_axis=0,
        tiled=True,
    )
    own_pair, near_pair, other_pair, far_pair = [
        shift(piece, partner) for piece in (out_weight, near, other, far)
    ]

    me = lax.axis_index("dp")
    x, core = me // 2, me % 2
    away = 1 - 2 * core
    steps = jnp.array([0, 1, -1, 0, 1, -1, 2, 2], jnp.int32) * away
    flips = jnp.array([0, 0, 0, 1, 1, 1, 0, 1], jnp.int32)
    columns = 2 * ((x + steps) % ring) + (core + flips) % 2
    pieces = [out_weight, other, near, own_pair, near_pair, other_pair, far, far_pair]
    mixed, normed, wire = project(
        columns, heads, pieces, residual[0], norm_gain.reshape(1, -1), place
    )
    wire_shape = (wire.shape[0] // 8, 8, wire.shape[1])

    def exchange(values):
        return lax.all_to_all(
            values.reshape(wire_shape), ("sp", "dp"), split_axis=0, concat_axis=0, tiled=True
        ).reshape(values.shape)

    arrived = exchange(wire)
    base = shared(normed, mixed, shared_gate, shared_up, shared_down)
    output = expert(arrived, expert_gate[0], expert_up[0], expert_down[0])
    returned = exchange(output)
    return combine(returned, gates, base).reshape(1, tokens, width)


def solution(mesh):
    in_specs = (
        P("dp", "sp", None),
        P("dp", "sp", None, None),
        P("dp", "sp", None, None),
        P(None, "dp"),
        P(),
        P(),
        P(),
        P("dp", "sp", None),
        P("dp", "sp", None),
        P(),
        P(),
        P(),
        P(("sp", "dp"), None, None),
        P(("sp", "dp"), None, None),
        P(("sp", "dp"), None, None),
    )
    out_specs = P("dp", "sp", None)
    return jax.shard_map(
        per_device, mesh=mesh, in_specs=in_specs, out_specs=out_specs, check_vma=False
    )
```

```python
import jax
import jax.numpy as jnp
import numpy as np
from jax import lax
from jax.experimental import pallas as pl
from jax.experimental.pallas import tpu as pltpu
from jax.sharding import PartitionSpec as P


GRID_W = 64
HD = 64
EPS = 1e-06
THETA = 10000.0
ROUTED_SCALE = 2.5
CAP = 6
PAIRS = CAP // 2
F32 = jnp.float32
BF16 = jnp.bfloat16


def iota(shape, axis):
    return lax.broadcasted_iota(jnp.int32, shape, axis)


LANES = 2 * HD


def local(values):
    return pltpu.with_memory_space_constraint(values, pltpu.VMEM)


def distant(values):
    return pltpu.with_memory_space_constraint(values, pltpu.HBM)


def limit(mib):
    return pltpu.CompilerParams(vmem_limit_bytes=mib * 2**20)


def angle_tables(tokens, blocks):
    lane = np.arange(LANES)
    by_row = lane % HD < HD // 2
    freq = THETA ** (-(2.0 * (lane % (HD // 4))) / (HD // 2))
    col = (np.arange(tokens) % GRID_W)[:, None] * freq[None, :]
    row = np.arange(blocks * tokens // GRID_W)[:, None] * freq[None, :]
    col = np.where(by_row, 0.0, np.stack([np.cos(col), np.sin(col)]))
    row = np.where(by_row, np.stack([np.cos(row), np.sin(row)]), 0.0)
    row = row.reshape(2, blocks, tokens // GRID_W, LANES).transpose(1, 0, 2, 3)
    return col.astype(np.float32), row.astype(np.float32)


def prepare_kernel(
    block_ref, q_ref, kv_ref, col_ref, row_ref, q_gain_ref, k_gain_ref, out_ref, table_ref
):
    del block_ref
    tokens, heads = q_ref.shape[:2]
    shape = (tokens, LANES)
    lane = iota(shape, 1)
    is_key = lane < HD
    block = (iota((LANES, LANES), 0) // HD == iota((LANES, LANES), 1) // HD).astype(F32).astype(BF16)

    @pl.when(pl.program_id(0) == 0)
    def _():
        lower = lane % (HD // 2) < HD // 4

        def angles(which):
            rows = [
                col_ref[which, r * GRID_W : (r + 1) * GRID_W, :] + row_ref[0, which, r : r + 1, :]
                for r in range(tokens // GRID_W)
            ]
            return jnp.concatenate(rows, axis=0)

        cosine, sine = angles(0), angles(1)

        def tables(gain_ref, scale):
            gain = gain_ref[...] * scale
            gain = jnp.broadcast_to(jnp.concatenate([gain, gain], axis=1), shape)
            up = pltpu.roll(gain, LANES - HD // 4, 1)
            down = pltpu.roll(gain, HD // 4, 1)
            return (
                gain * cosine,
                jnp.where(lower, -up * sine, 0.0),
                jnp.where(lower, 0.0, down * sine),
            )

        for i, table in enumerate(tables(q_gain_ref, HD**-0.5)):
            table_ref[i] = table
        own, up, down = tables(k_gain_ref, 1.0)
        table_ref[3] = jnp.where(is_key, own, 1.0)
        table_ref[4] = jnp.where(is_key, up, 0.0)
        table_ref[5] = jnp.where(is_key, down, 0.0)

    def turned(x, base, keys):
        square = x * x
        high = square.astype(BF16)
        low = (square - high.astype(F32)).astype(BF16)
        total = jnp.dot(high, block, preferred_element_type=F32)
        total = total + jnp.dot(low, block, preferred_element_type=F32)
        scale = lax.rsqrt(total * (1.0 / HD) + EPS)
        if keys:
            scale = jnp.where(is_key, scale, 1.0)
        mixed = (
            x * table_ref[base]
            + pltpu.roll(x, LANES - HD // 4, 1) * table_ref[base + 1]
            + pltpu.roll(x, HD // 4, 1) * table_ref[base + 2]
        )
        return (mixed * scale).astype(BF16)

    query = jnp.swapaxes(q_ref[...].astype(F32), 0, 1)
    pair = jnp.swapaxes(kv_ref[...].astype(F32), 0, 1)
    for h in range(heads):
        out_ref[h, :, :LANES] = turned(query[h], 0, False)
        out_ref[h, :, LANES:] = turned(pair[h], 3, True)


def prepare(query, pair, query_gain, key_gain, block, blocks):
    tokens, heads, width = query.shape
    step = 8
    col, row = angle_tables(tokens, blocks)
    gains = [gain.reshape(1, -1) for gain in (query_gain, key_gain)]
    return pl.pallas_call(
        prepare_kernel,
        grid_spec=pltpu.PrefetchScalarGridSpec(
            num_scalar_prefetch=1,
            grid=(heads // step,),
            in_specs=[
                pl.BlockSpec((tokens, step, width), lambda i, b: (0, i, 0)),
                pl.BlockSpec((tokens, step, width), lambda i, b: (0, i, 0)),
                pl.BlockSpec(col.shape, lambda i, b: (0, 0, 0)),
                pl.BlockSpec((1,) + row.shape[1:], lambda i, b: (b[0], 0, 0, 0)),
                pl.BlockSpec((1, HD), lambda i, b: (0, 0)),
                pl.BlockSpec((1, HD), lambda i, b: (0, 0)),
            ],
            out_specs=pl.BlockSpec((step, tokens, 2 * width), lambda i, b: (i, 0, 0)),
            scratch_shapes=[pltpu.VMEM((6, tokens, width), F32)],
        ),
        out_shape=jax.ShapeDtypeStruct((heads, tokens, 2 * width), BF16),
        compiler_params=limit(16),
        name="prepare",
    )(
        jnp.full((1,), block, jnp.int32),
        *(distant(array) for array in (query, pair, jnp.asarray(col), jnp.asarray(row), *gains)),
    )


def attend_kernel(q_ref, kv_ref, out_ref, keys_ref, values_ref):
    @pl.when(pl.program_id(0) == 0)
    def _():
        key = kv_ref[:, 128 : 128 + HD]
        value = kv_ref[:, 128 + HD :]
        keys_ref[...] = jnp.concatenate([key, key], axis=1)
        values_ref[:, :128] = jnp.concatenate([value, value], axis=1)
        values_ref[:, 128:] = jnp.ones_like(values_ref[:, 128:])

    first = iota((1, 128), 1) < HD
    block = 1024
    parts = [(r, head) for r in range(q_ref.shape[0] // block) for head in range(2)]

    def score(part):
        r, head = part
        query = q_ref[r * block : (r + 1) * block, :]
        mine = jnp.where(first if head == 0 else ~first, query, jnp.zeros_like(query))
        return lax.dot_general(
            mine, keys_ref[...], (((1,), (1,)), ((), ())), preferred_element_type=F32
        )

    def mix(scores):
        weights = jnp.exp(scores - jnp.max(scores, axis=-1, keepdims=True)).astype(BF16)
        mixed = jnp.dot(weights, values_ref[...], preferred_element_type=F32)
        return mixed[:, :128] / mixed[:, 128:]

    outs = []
    ahead = score(parts[0])
    for n in range(len(parts)):
        scores = ahead
        if n + 1 < len(parts):
            ahead = score(parts[n + 1])
        outs.append(mix(scores))
    for r in range(len(parts) // 2):
        out_ref[r * block : (r + 1) * block, :] = jnp.where(
            first, outs[2 * r], outs[2 * r + 1]
        ).astype(BF16)


def attend(rows):
    length, width = rows.shape
    block = 1024
    return pl.pallas_call(
        attend_kernel,
        grid=(length // block,),
        in_specs=[
            pl.BlockSpec((block, 128), lambda i: (i, 0)),
            pl.BlockSpec((length, width), lambda i: (0, 0)),
        ],
        out_specs=pl.BlockSpec((block, 128), lambda i: (i, 0)),
        out_shape=pltpu.HBM((length, 128), BF16),
        scratch_shapes=[pltpu.VMEM((length, 128), BF16), pltpu.VMEM((length, 256), BF16)],
        compiler_params=limit(32),
        name="attend",
    )(rows, rows)


def route_kernel(ids_ref, weights_ref, place_ref, gates_ref):
    tokens, top = ids_ref.shape
    experts = place_ref.shape[0] // CAP
    expert = iota((tokens, experts), 1)
    hits = [(ids_ref[:, k : k + 1] == expert).astype(F32) for k in range(top)]
    used = sum(hits[1:], hits[0])
    earlier = (iota((tokens, tokens), 1) < iota((tokens, tokens), 0)).astype(F32).astype(BF16)
    before = jnp.dot(earlier, used.astype(BF16), preferred_element_type=F32)
    raw = weights_ref[...]
    gate = raw / jnp.sum(raw, axis=-1, keepdims=True) * ROUTED_SCALE
    slots = iota((tokens, experts * CAP), 1)
    place = jnp.zeros((tokens, experts * CAP), F32)
    gated = jnp.zeros((tokens, experts * CAP), F32)
    for k in range(top):
        rank = jnp.sum(hits[k] * before, axis=-1, keepdims=True).astype(jnp.int32)
        slot = rank * experts + ids_ref[:, k : k + 1]
        here = slots == slot
        place = jnp.where(here, 1.0, place)
        gated = jnp.where(here, gate[:, k : k + 1], gated)
    place_ref[...] = jnp.transpose(place).astype(BF16)
    gates_ref[...] = gated


def route(ids, weights, experts):
    tokens, _ = ids.shape
    return pl.pallas_call(
        route_kernel,
        out_shape=(
            pltpu.VMEM((experts * CAP, tokens), BF16),
            pltpu.VMEM((tokens, experts * CAP), F32),
        ),
        compiler_params=limit(8),
        name="route",
    )(ids, weights)


CHUNKS = 8


def fold(rows, wire_ref, slot):
    peers, width = rows.shape
    for half in range(width // (CHUNKS * 128)):
        first = half * CHUNKS * 128
        chunks = jnp.stack(
            [rows[:, first + n * 128 : first + (n + 1) * 128] for n in range(CHUNKS)]
        )
        block = jnp.swapaxes(chunks, 0, 1).reshape(peers * CHUNKS, 128)
        lane = (slot * (width // (CHUNKS * 128)) + half) * 128
        wire_ref[:, lane : lane + 128] = block.astype(BF16)


def unfold(wire_ref, rows_ref):
    group = 128 // CHUNKS
    peers = wire_ref.shape[0] // CHUNKS
    halves = rows_ref.shape[1] // (CHUNKS * 128)
    sent, kept = iota((128, 128), 1), iota((128, 128), 0)
    permute = (sent == kept % group * CHUNKS + kept // group).astype(F32).astype(BF16)
    for g in range(peers // group):
        block = jnp.dot(
            permute, wire_ref[g * 128 : (g + 1) * 128, :], preferred_element_type=F32
        ).astype(BF16)
        for slot in range(CAP):
            first = slot * peers + g * group
            for chunk in range(halves * CHUNKS):
                lane = (slot * halves + chunk // CHUNKS) * 128
                row = chunk % CHUNKS * group
                rows_ref[first : first + group, chunk * 128 : (chunk + 1) * 128] = block[
                    row : row + group, lane : lane + 128
                ]


def unfold_slots(wire_ref, rows_ref, slots):
    peers = wire_ref.shape[0] // CHUNKS
    halves = rows_ref.shape[1] // (CHUNKS * 128)
    for slot in slots:
        for half in range(halves):
            lane = (slot * halves + half) * 128
            block = wire_ref[:, lane : lane + 128].astype(F32).reshape(peers, CHUNKS, 128)
            chunks = jnp.swapaxes(block, 0, 1).astype(BF16)
            for n in range(CHUNKS):
                at = (half * CHUNKS + n) * 128
                rows_ref[slot * peers : (slot + 1) * peers, at : at + 128] = chunks[n]


def project_kernel(columns_ref, heads_ref, *refs):
    placed, pieces = refs[:2], refs[2:8]
    residual_hbm, gain_ref, place_ref, mixed_hbm, normed_hbm, wire_ref = refs[8:14]
    weight_ref, residual_ref, part_ref, mixed_ref, normed_ref, sems = refs[14:]
    copies = [
        pltpu.make_async_copy(pieces[s], weight_ref.at[s], sems.at[s]) for s in range(6)
    ]
    copies.append(pltpu.make_async_copy(residual_hbm, residual_ref, sems.at[6]))
    copies.append(pltpu.make_async_copy(mixed_ref, mixed_hbm, sems.at[7]))
    copies.append(pltpu.make_async_copy(normed_ref, normed_hbm, sems.at[8]))
    for copy in copies[:7]:
        copy.start()
    rows = jnp.concatenate([heads_ref[h] for h in range(heads_ref.shape[0])], axis=1)
    for s in range(8):
        if s >= 2:
            copies[s - 2].wait()
        weight = weight_ref[s - 2] if s >= 2 else placed[s][...]
        part_ref[columns_ref[s]] = jnp.dot(rows, weight, preferred_element_type=F32)
    copies[6].wait()
    width = part_ref.shape[2]
    square = None
    for j in range(8):
        block = part_ref[j] + residual_ref[:, j * width : (j + 1) * width].astype(F32)
        mixed_ref[:, j * width : (j + 1) * width] = block
        part = jnp.sum(block * block, axis=-1, keepdims=True)
        square = part if square is None else square + part
    scale = lax.rsqrt(square * (1.0 / (8 * width)) + EPS)
    normed = (mixed_ref[...] * scale * gain_ref[...]).astype(BF16)
    normed_ref[...] = normed
    copies[7].start()
    copies[8].start()
    peers = place_ref.shape[0] // CAP
    for slot in range(CAP):
        rows = jnp.dot(
            place_ref[slot * peers : (slot + 1) * peers, :], normed, preferred_element_type=F32
        )
        fold(rows, wire_ref, slot)
    copies[7].wait()
    copies[8].wait()


def project(columns, heads, pieces, residual, gain, place):
    tokens, width = residual.shape
    peers = place.shape[0] // CAP
    vmem = pl.BlockSpec(memory_space=pltpu.VMEM)
    return pl.pallas_call(
        project_kernel,
        in_specs=[pl.BlockSpec(memory_space=pltpu.SMEM)]
        + [vmem] * 3
        + [pl.BlockSpec(memory_space=pl.ANY)] * 7
        + [vmem] * 2,
        out_specs=[pl.BlockSpec(memory_space=pl.ANY)] * 2 + [vmem],
        out_shape=(
            pltpu.HBM((tokens, width), F32),
            pltpu.HBM((tokens, width), BF16),
            pltpu.VMEM((peers * 8, width * CAP // 8), BF16),
        ),
        scratch_shapes=[
            pltpu.VMEM((6,) + pieces[0].shape, BF16),
            pltpu.VMEM(residual.shape, BF16),
            pltpu.VMEM((8, tokens, width // 8), F32),
            pltpu.VMEM((tokens, width), F32),
            pltpu.VMEM((tokens, width), BF16),
            pltpu.SemaphoreType.DMA((9,)),
        ],
        compiler_params=limit(24),
        name="project",
    )(
        columns,
        local(heads),
        *(local(piece) for piece in pieces[:2]),
        *(distant(piece) for piece in pieces[2:]),
        distant(residual),
        gain,
        local(place),
    )


def expert_kernel(wire_ref, gate_ref, up_ref, down_ref, out_hbm, rows_ref, out_ref, sems):
    peers = rows_ref.shape[0] // CAP
    part = out_ref.shape[1] // PAIRS
    copies = []

    def finish(c, output):
        fold(output[:peers], out_ref, 2 * c)
        fold(output[peers:], out_ref, 2 * c + 1)
        lanes = pl.ds(c * part, part)
        copies.append(
            pltpu.make_async_copy(out_ref.at[:, lanes], out_hbm.at[:, lanes], sems.at[c])
        )
        copies[c].start()

    def hidden_of(rows):
        gate = jnp.dot(rows, gate_ref[...], preferred_element_type=F32)
        up = jnp.dot(rows, up_ref[...], preferred_element_type=F32)
        return (gate / (1.0 + jnp.exp(-gate)) * up).astype(BF16)

    def output_of(hidden):
        return jnp.dot(hidden, down_ref[...], preferred_element_type=F32)

    unfold_slots(wire_ref, rows_ref, range(CAP))
    hidden = hidden_of(rows_ref[...])
    for c in range(PAIRS):
        finish(c, output_of(hidden[c * 2 * peers : (c + 1) * 2 * peers]))
    for copy in copies:
        copy.wait()


def expert(wire, gate, up, down):
    rows, width = wire.shape
    vmem = pl.BlockSpec(memory_space=pltpu.VMEM)
    return pl.pallas_call(
        expert_kernel,
        in_specs=[vmem] * 4,
        out_specs=pl.BlockSpec(memory_space=pl.ANY),
        out_shape=pltpu.HBM(wire.shape, BF16),
        scratch_shapes=[
            pltpu.VMEM((rows * CAP // 8, width * 8 // CAP), BF16),
            pltpu.VMEM(wire.shape, BF16),
            pltpu.SemaphoreType.DMA((PAIRS,)),
        ],
        compiler_params=limit(32),
        name="expert",
    )(local(wire), local(gate), local(up), local(down))


def shared_kernel(normed_ref, mixed_ref, gate_ref, up_ref, down_ref, out_ref):
    rows = normed_ref[...]
    gate = jnp.dot(rows, gate_ref[...], preferred_element_type=F32)
    up = jnp.dot(rows, up_ref[...], preferred_element_type=F32)
    hidden = (gate / (1.0 + jnp.exp(-gate)) * up).astype(BF16)
    output = jnp.dot(hidden, down_ref[...], preferred_element_type=F32)

    @pl.when(pl.program_id(0) == 0)
    def _():
        out_ref[...] = mixed_ref[...] + output

    @pl.when(pl.program_id(0) > 0)
    def _():
        out_ref[...] = out_ref[...] + output


def shared(normed, mixed, gate, up, down):
    block = 256

    def whole(array):
        return pl.BlockSpec(array.shape, lambda i: (0, 0))

    columns = pl.BlockSpec((gate.shape[0], block), lambda i: (0, i))
    return pl.pallas_call(
        shared_kernel,
        grid=(gate.shape[1] // block,),
        in_specs=[
            whole(normed),
            whole(mixed),
            columns,
            columns,
            pl.BlockSpec((block, down.shape[1]), lambda i: (i, 0)),
        ],
        out_specs=whole(mixed),
        out_shape=pltpu.HBM(mixed.shape, F32),
        compiler_params=limit(20),
        name="shared",
    )(*(distant(array) for array in (normed, mixed, gate, up, down)))


def combine_kernel(wire_ref, gates_ref, base_hbm, out_hbm, rows_ref, base_ref, out_ref, sems):
    blocks = sems.shape[0] - 1
    block = base_ref.shape[1] // blocks
    fetch = pltpu.make_async_copy(base_hbm, base_ref, sems.at[blocks])
    fetch.start()
    gates = gates_ref[...]
    tokens = gates.shape[0]
    high = gates.astype(BF16)
    low = (gates - high.astype(F32)).astype(BF16)
    stacked = jnp.concatenate([high, low], axis=0)
    unfold(wire_ref, rows_ref)
    fetch.wait()
    copies = []
    for n in range(blocks):
        lanes = slice(n * block, (n + 1) * block)
        parts = jnp.dot(stacked, rows_ref[:, lanes], preferred_element_type=F32)
        routed = parts[:tokens] + parts[tokens:]
        out_ref[:, lanes] = (base_ref[:, lanes] + routed).astype(BF16)
        lanes = pl.ds(n * block, block)
        copies.append(
            pltpu.make_async_copy(out_ref.at[:, lanes], out_hbm.at[:, lanes], sems.at[n])
        )
        copies[n].start()
    for copy in copies:
        copy.wait()


def combine(wire, gates, base):
    rows, width = wire.shape
    vmem = pl.BlockSpec(memory_space=pltpu.VMEM)
    return pl.pallas_call(
        combine_kernel,
        in_specs=[vmem, vmem, pl.BlockSpec(memory_space=pl.ANY)],
        out_specs=pl.BlockSpec(memory_space=pl.ANY),
        out_shape=pltpu.HBM(base.shape, BF16),
        scratch_shapes=[
            pltpu.VMEM((rows * CAP // 8, width * 8 // CAP), BF16),
            pltpu.VMEM(base.shape, F32),
            pltpu.VMEM(base.shape, BF16),
            pltpu.SemaphoreType.DMA((5,)),
        ],
        compiler_params=limit(24),
        name="combine",
    )(local(wire), local(gates), distant(base))


def shift(values, target):
    size = lax.axis_size("dp")

    def place(d):
        x, core = target(d // 2, d % 2)
        return 2 * (x % (size // 2)) + core

    return lax.ppermute(values, "dp", [(d, place(d)) for d in range(size)])


def apart(x, core):
    return x + 1 - 2 * core, core


def across(x, core):
    return x - 1 + 2 * core, core


def partner(x, core):
    return x, 1 - core


def per_device(
    residual,
    query,
    key_value,
    out_weight,
    norm_gain,
    query_gain,
    key_gain,
    route_ids,
    route_weights,
    shared_gate,
    shared_up,
    shared_down,
    expert_gate,
    expert_up,
    expert_down,
):
    tokens, width = residual.shape[1:]
    experts = expert_gate.shape[0] * lax.axis_size(("sp", "dp"))
    ring = lax.axis_size("dp") // 2
    blocks = lax.axis_size("sp")

    near = shift(out_weight, apart)
    other = shift(out_weight, across)
    outgoing = prepare(query[0], key_value[0], query_gain, key_gain, lax.axis_index("sp"), blocks)
    rows = lax.all_to_all(outgoing, "sp", split_axis=0, concat_axis=0, tiled=True)
    rows, near, other = lax.optimization_barrier((rows, near, other))
    far = shift(near, apart)
    attention = attend(rows.reshape(-1, rows.shape[2]))
    place, gates = route(route_ids[0], route_weights[0], experts)
    heads = lax.all_to_all(
        attention.reshape(-1, tokens, attention.shape[1]),
        "sp",
        split_axis=0,
        concat_axis=0,
        tiled=True,
    )
    own_pair, near_pair, other_pair, far_pair = [
        shift(piece, partner) for piece in (out_weight, near, other, far)
    ]

    me = lax.axis_index("dp")
    x, core = me // 2, me % 2
    away = 1 - 2 * core
    steps = jnp.array([0, 1, -1, 0, 1, -1, 2, 2], jnp.int32) * away
    flips = jnp.array([0, 0, 0, 1, 1, 1, 0, 1], jnp.int32)
    columns = 2 * ((x + steps) % ring) + (core + flips) % 2
    pieces = [out_weight, other, near, own_pair, near_pair, other_pair, far, far_pair]
    mixed, normed, wire = project(
        columns, heads, pieces, residual[0], norm_gain.reshape(1, -1), place
    )
    wire_shape = (wire.shape[0] // 8, 8, wire.shape[1])

    def exchange(values):
        return lax.all_to_all(
            values.reshape(wire_shape), ("sp", "dp"), split_axis=0, concat_axis=0, tiled=True
        ).reshape(values.shape)

    arrived = exchange(wire)
    base = shared(normed, mixed, shared_gate, shared_up, shared_down)
    output = expert(arrived, expert_gate[0], expert_up[0], expert_down[0])
    returned = exchange(output)
    return combine(returned, gates, base).reshape(1, tokens, width)


def solution(mesh):
    in_specs = (
        P("dp", "sp", None),
        P("dp", "sp", None, None),
        P("dp", "sp", None, None),
        P(None, "dp"),
        P(),
        P(),
        P(),
        P("dp", "sp", None),
        P("dp", "sp", None),
        P(),
        P(),
        P(),
        P(("sp", "dp"), None, None),
        P(("sp", "dp"), None, None),
        P(("sp", "dp"), None, None),
    )
    out_specs = P("dp", "sp", None)
    return jax.shard_map(
        per_device, mesh=mesh, in_specs=in_specs, out_specs=out_specs, check_vma=False
    )
```
